512 devices in a mesh: fs: 64 (over z, y), tp: 8 (over x, core).
Axes of the slice: x: 4, y: 4, z: 16, core: 2. Of those that a mesh axis runs over, the one named last changes fastest.
Arguments:
- tokens: bfloat16 [32768, 2048], P('fs', 'tp'), may hold values from -6 to 6
- norm_gain: bfloat16 [2048], P('tp'), may hold values from 0.099609375 to 1.8984375
- proj_u: bfloat16 [2048, 2048], P('fs', 'tp'), may hold values from -0.125 to 0.125
- proj_v: bfloat16 [2048, 2048], P('fs', 'tp'), may hold values from -0.125 to 0.125
- layer_gain: bfloat16 [2048], P('tp'), may hold values from 0.099609375 to 1.8984375
- layer_shift: bfloat16 [2048], P('tp'), may hold values from -3 to 3
- mix_weight: bfloat16 [16, 128, 128], P('tp'), may hold values from -0.5 to 0.5
- mix_bias: bfloat16 [16, 128], P('tp'), may hold values from 0.099609375 to 1.8984375
- proj_out: bfloat16 [2048, 2048], P('tp', 'fs'), may hold values from -0.375 to 0.375
- ffn_gain: bfloat16 [2048], P('tp'), may hold values from 0.099609375 to 1.8984375
- ffn_gate: bfloat16 [2048, 4096], P('fs', 'tp'), may hold values from -0.125 to 0.125
- ffn_value: bfloat16 [2048, 4096], P('fs', 'tp'), may hold values from -0.125 to 0.125
- conv_gate: bfloat16 [3, 4096], P(None, 'tp'), may hold values from -3 to 3
- conv_value: bfloat16 [3, 4096], P(None, 'tp'), may hold values from -3 to 3
- proj_down: bfloat16 [4096, 2048], P('tp', 'fs'), may hold values from -0.25 to 0.25
Outputs:
- result: bfloat16 [32768, 2048], P('fs', 'tp')
The draws below stay inside these ranges and needn't reach their ends.
All inputs are finite; a program needn't handle non-finite values.
Results may differ from the reference program's by a relative error of at most 0.017.
Values may be sent and summed in bfloat16 or wider, within the bound.
No kernel may reach another device: no remote copies, remote signals or barrier semaphores. Data moves between devices by JAX's collectives and lax.ppermute only.
A program may use at most 64 MiB of HBM per device.

```python
import jax
import jax.numpy as jnp
from jax import lax

D = 2048
GROUPS = 16
GROUP_DIM = 128
DA = 2048
FF = 4096
BLOCK = 128
SEGMENT = 64
KERNEL = 3
SEQ_LEN = 256
TOK_DEV = 512
TOKENS = 32768
N_FS = 64
N_TP = 8


def draw_tokens(key, part):
    column = jnp.arange(D).astype(jnp.float32)
    col_scale = 0.6 * 3.0 ** (column / D)
    values = jax.random.normal(key, (TOKENS, D), jnp.float32) * col_scale
    return jnp.clip(values, -6.0, 6.0).astype(jnp.bfloat16)


def strengthened(drawn, stream_key, source, target, blocks, factor):
    owner, partner = [(jnp.arange(drawn.shape[dim]) // (drawn.shape[dim] // blocks)).reshape([-1 if axis == dim else 1 for axis in range(drawn.ndim)]) for dim in (source, target)]
    chosen = jax.random.permutation(stream_key, blocks)[partner]
    strong = (owner == chosen) | (owner == (partner + blocks // 2) % blocks)
    return jnp.where(strong, factor * drawn, drawn)


def levels(own_key, shape, shards, least, high):
    factor_of, own = 1.0, jax.random.fold_in(own_key, 6)
    for position, blocks in shards:
        draws = jnp.exp(jax.random.uniform(jax.random.fold_in(own, position), (blocks,), jnp.float32, least / len(shards), high / len(shards)))
        factor_of = factor_of * jnp.repeat(draws, shape[position] // blocks).reshape([-1 if axis == position else 1 for axis in range(len(shape))])
    return factor_of


def bell_draw(key, extent, scale, most, cuts=(), dtype=jnp.bfloat16):
    loudness = levels(key, extent, cuts, -0.22, 0.18) if cuts else 1.0
    values = jax.random.normal(key, extent, jnp.float32) * scale * loudness
    return jnp.minimum(jnp.maximum(values, -most), most).astype(dtype)


def bell_draw_with(own_key, dims, scale, most, cuts, heavy, dtype=jnp.bfloat16):
    array = scale * jax.random.normal(own_key, dims, jnp.float32)
    if cuts:
        array = array * levels(own_key, dims, cuts, -0.22, 0.18)
    return jnp.clip(strengthened(array, jax.random.fold_in(own_key, 3), *heavy), -most, most).astype(dtype)


def setup_inputs(seed: int = 0) -> dict:
    keys = jax.random.split(jax.random.key(seed), 16)
    tokens = draw_tokens(jax.random.fold_in(keys[15], 71), 0)
    norm_gain = jnp.clip(1.0 + 0.18 * jax.random.normal(keys[1], (D,), jnp.float32), 0.099609375, 1.8984375).astype(jnp.bfloat16)
    proj_u = bell_draw(keys[2], (D, DA), D ** -0.5, 0.125, ((0, 64), (1, 8)))
    proj_v = bell_draw(keys[3], (D, DA), D ** -0.5, 0.125, ((0, 64), (1, 8)))
    layer_gain = jnp.clip(1.0 + 0.18 * jax.random.normal(keys[4], (DA,), jnp.float32), 0.099609375, 1.8984375).astype(jnp.bfloat16)
    layer_shift = bell_draw(keys[5], (DA,), 0.5, 3.0, ((0, 8),))
    mix_weight = bell_draw(keys[6], (GROUPS, BLOCK, BLOCK), BLOCK ** -0.5, 0.5, ((0, 8),))
    mix_bias = jnp.clip(1.0 + 0.18 * jax.random.normal(keys[7], (GROUPS, BLOCK), jnp.float32), 0.099609375, 1.8984375).astype(jnp.bfloat16)
    proj_out = bell_draw_with(keys[8], (DA, D), DA ** -0.5, 0.375, ((0, 8), (1, 64)), (0, 1, 64, 4.0))
    ffn_gain = jnp.clip(1.0 + 0.18 * jax.random.normal(keys[9], (D,), jnp.float32), 0.099609375, 1.8984375).astype(jnp.bfloat16)
    ffn_gate = bell_draw(keys[10], (D, FF), D ** -0.5, 0.125, ((0, 64), (1, 8)))
    ffn_value = bell_draw(keys[11], (D, FF), D ** -0.5, 0.125, ((0, 64), (1, 8)))
    conv_gate = bell_draw(keys[12], (KERNEL, FF), 0.6, 3.0, ((1, 8),))
    conv_value = bell_draw(keys[13], (KERNEL, FF), 0.6, 3.0, ((1, 8),))
    proj_down = bell_draw_with(keys[14], (FF, D), FF ** -0.5, 0.25, ((0, 8), (1, 64)), (0, 1, 64, 4.0))
    return dict(tokens=tokens, norm_gain=norm_gain, proj_u=proj_u, proj_v=proj_v, layer_gain=layer_gain, layer_shift=layer_shift, mix_weight=mix_weight, mix_bias=mix_bias, proj_out=proj_out, ffn_gain=ffn_gain, ffn_gate=ffn_gate, ffn_value=ffn_value, conv_gate=conv_gate, conv_value=conv_value, proj_down=proj_down)


EPS = 1e-06

def matmul(operand, matrix):
    return jnp.dot(operand, matrix, preferred_element_type=jnp.float32)

def share_sum(operand, matrix, share_width):
    summed = jnp.zeros((operand.shape[0], matrix.shape[1]), jnp.float32)
    for index in range(N_TP):
        lower = index * share_width
        product = matmul(operand[:, lower:lower + share_width], matrix[lower:lower + share_width, :])
        rounded = lax.optimization_barrier(product.astype(jnp.bfloat16))
        summed = summed + rounded.astype(jnp.float32)
    return summed

def rms_rows(values_in, gain_row):
    values = values_in.astype(jnp.float32)
    scale_row = lax.rsqrt(lax.optimization_barrier(jnp.mean(values * values, axis=1, keepdims=True)) + EPS)
    return (values * scale_row * gain_row.astype(jnp.float32)).astype(jnp.bfloat16)

def causal_taps(values, weights):
    seq_count = values.shape[0] // SEQ_LEN
    shaped = values.reshape(seq_count, SEQ_LEN, values.shape[1])
    padded = jnp.pad(shaped, ((0, 0), (KERNEL - 1, 0), (0, 0)))
    summed = jnp.zeros(shaped.shape, jnp.float32)
    for tap_index in range(KERNEL):
        summed = summed + padded[:, tap_index:tap_index + SEQ_LEN].astype(jnp.float32) * weights[tap_index].astype(jnp.float32)
    return summed.reshape(values.shape[0], values.shape[1])

def reference(tokens, norm_gain, proj_u, proj_v, layer_gain, layer_shift, mix_weight, mix_bias, proj_out, ffn_gain, ffn_gate, ffn_value, conv_gate, conv_value, proj_down):
    segment = jnp.arange(BLOCK) // SEGMENT
    visible = segment[None, :] <= segment[:, None]
    masked = jnp.where(visible[None], mix_weight, jnp.zeros_like(mix_weight)).astype(jnp.float32)

    def one_block(token_rows):
        row_count = token_rows.shape[0]
        normed = rms_rows(token_rows, norm_gain)
        act_u = jax.nn.gelu(matmul(normed, proj_u), approximate=False)
        act_v = jax.nn.gelu(matmul(normed, proj_v), approximate=False)
        center = lax.optimization_barrier(jnp.mean(act_v, axis=1, keepdims=True))
        spread = lax.optimization_barrier(jnp.mean(act_v * act_v, axis=1, keepdims=True)) - center * center
        mixed_in = ((act_v - center) * lax.rsqrt(spread + EPS) * layer_gain.astype(jnp.float32) + layer_shift.astype(jnp.float32)).astype(jnp.bfloat16)
        blocks = mixed_in.reshape(row_count // BLOCK, BLOCK, GROUPS, GROUP_DIM).astype(jnp.float32)
        spatial = jnp.einsum('gij,njgc->nigc', masked, blocks) + mix_bias.astype(jnp.float32).T[None, :, :, None]
        gated = (act_u * spatial.reshape(row_count, DA)).astype(jnp.bfloat16)
        stream = (token_rows.astype(jnp.float32) + share_sum(gated, proj_out, DA // N_TP)).astype(jnp.bfloat16)
        normed_two = rms_rows(stream, ffn_gain)
        up_gate = matmul(normed_two, ffn_gate).astype(jnp.bfloat16)
        up_value = matmul(normed_two, ffn_value).astype(jnp.bfloat16)
        conv_g = causal_taps(up_gate, conv_gate)
        conv_v = causal_taps(up_value, conv_value)
        hidden = (jax.nn.silu(conv_g) * conv_v).astype(jnp.bfloat16)
        return (stream.astype(jnp.float32) + share_sum(hidden, proj_down, FF // N_TP)).astype(jnp.bfloat16)
    grouped = tokens.reshape(N_FS, TOK_DEV, D)
    return lax.map(one_block, grouped).reshape(TOKENS, D)
```

```python
import jax
import jax.numpy as jnp
from jax import lax
from jax.sharding import Mesh
from jax.sharding import PartitionSpec as P

GROUP_DIM = 128
BLOCK = 128
SEGMENT = 64
KERNEL = 3
SEQ_LEN = 256
FS = ("z", "y")
TP = ("x", "c")
EPS = 1e-06
F32 = jnp.float32
BF16 = jnp.bfloat16
SWAP = [(0, 1), (1, 0)]


def everyones(shard, axis):
    copies = jnp.broadcast_to(shard, (lax.axis_size(axis), *shard.shape))
    return lax.all_to_all(copies, axis, split_axis=0, concat_axis=0, tiled=True)


def other_core(value):
    return lax.ppermute(value, "c", SWAP)


def matmul(operand, matrix):
    return jnp.dot(operand, matrix, preferred_element_type=F32)


def matmul_t(operand, matrix):
    return lax.dot_general(operand, matrix, (((1,), (1,)), ((), ())), preferred_element_type=F32)


def whole_rows(shard):
    n, w = shard.shape
    mine = everyones(shard, "x")
    other = other_core(mine)
    first = lax.axis_index("c") == 0
    both = jnp.stack([jnp.where(first, mine, other), jnp.where(first, other, mine)], axis=1)
    return both.reshape(-1, n, w).transpose(1, 0, 2).reshape(n, -1)


def rms(values, gain):
    v = values.astype(F32)
    scale = lax.rsqrt(jnp.mean(v * v, axis=1, keepdims=True) + EPS)
    return (v * scale * gain.astype(F32)).astype(BF16)


def causal_taps(values, weights):
    seq_count = values.shape[0] // SEQ_LEN
    shaped = values.reshape(seq_count, SEQ_LEN, values.shape[1])
    padded = jnp.pad(shaped, ((0, 0), (KERNEL - 1, 0), (0, 0)))
    summed = jnp.zeros(shaped.shape, F32)
    for k in range(KERNEL):
        summed = summed + padded[:, k : k + SEQ_LEN].astype(F32) * weights[k].astype(F32)
    return summed.reshape(values.shape[0], values.shape[1])


def product_at_owner(rows, matrix):
    blocks = matrix.reshape(lax.axis_size("x"), 2, -1, matrix.shape[1])
    first = lax.axis_index("c") == 0
    keep = jnp.where(first, blocks[:, 0], blocks[:, 1])
    give = jnp.where(first, blocks[:, 1], blocks[:, 0])
    width = keep.shape[1]

    def split(w):
        return matmul_t(rows, w.reshape(-1, w.shape[2])).astype(BF16)

    came = other_core(split(give))
    pair = (split(keep).astype(F32) + came.astype(F32)).astype(BF16)
    parts = pair.reshape(rows.shape[0], -1, width).transpose(1, 0, 2)
    arrived = lax.all_to_all(parts, "x", split_axis=0, concat_axis=0, tiled=True)
    return arrived.astype(F32).sum(axis=0)


def on_device(
    tokens,
    norm_gain,
    proj_u,
    proj_v,
    layer_gain,
    layer_shift,
    mix_weight,
    mix_bias,
    proj_out,
    ffn_gain,
    ffn_gate,
    ffn_value,
    conv_gate,
    conv_value,
    proj_down,
):
    da = proj_u.shape[1]
    ff = ffn_gate.shape[1]
    row_count = tokens.shape[0]

    late = jnp.concatenate([ffn_gate, ffn_value, proj_down.T], axis=1)
    late_y = everyones(late, "y").reshape(-1, late.shape[1])
    late_all = lax.all_gather(late_y, "z", axis=0, tiled=True)

    early = jnp.concatenate([proj_u, proj_v, proj_out.T], axis=1)
    early_z = everyones(early, "z")
    packed = jnp.concatenate([tokens, jnp.broadcast_to(norm_gain, (8, da)), jnp.broadcast_to(ffn_gain, (8, da))], axis=0)
    whole = whole_rows(packed)
    normed = rms(whole[:row_count], whole[row_count])
    gain_two = whole[row_count + 8]
    early_all = everyones(early_z, "y").transpose(1, 0, 2, 3).reshape(-1, early.shape[1])

    act_v = jax.nn.gelu(matmul(normed, early_all[:, da : 2 * da]), approximate=False)
    sums = jnp.stack([jnp.sum(act_v, axis=1), jnp.sum(act_v * act_v, axis=1)])
    totals = everyones(sums.reshape(-1), TP).sum(axis=0).reshape(2, -1)
    act_u = jax.nn.gelu(matmul(normed, early_all[:, :da]), approximate=False)
    full_width = da * lax.axis_size(TP)
    center = totals[0] / full_width
    spread = totals[1] / full_width - center * center
    mixed_in = (
        (act_v - center[:, None]) * lax.rsqrt(spread + EPS)[:, None] * layer_gain.astype(F32) + layer_shift.astype(F32)
    ).astype(BF16)
    groups = da // GROUP_DIM
    blocks = mixed_in.reshape(row_count // BLOCK, BLOCK, groups, GROUP_DIM)
    segment = jnp.arange(BLOCK) // SEGMENT
    visible = segment[None, :] <= segment[:, None]
    masked = jnp.where(visible[None], mix_weight, jnp.zeros_like(mix_weight))
    spatial = (
        jnp.einsum("gij,njgc->nigc", masked, blocks, preferred_element_type=F32)
        + mix_bias.astype(F32).T[None, :, :, None]
    )
    gated = (act_u * spatial.reshape(row_count, da)).astype(BF16)
    stream = (tokens.astype(F32) + product_at_owner(gated, early_all[:, 2 * da :])).astype(BF16)
    normed_two = rms(whole_rows(stream), gain_two)
    pre_gate = matmul(normed_two, late_all[:, :ff]).astype(BF16)
    pre_value = matmul(normed_two, late_all[:, ff : 2 * ff]).astype(BF16)
    conv_g = causal_taps(pre_gate, conv_gate)
    conv_v = causal_taps(pre_value, conv_value)
    hidden = (jax.nn.silu(conv_g) * conv_v).astype(BF16)
    return (stream.astype(F32) + product_at_owner(hidden, late_all[:, 2 * ff :])).astype(BF16)


def solution(mesh):
    split = Mesh(mesh.devices.reshape(16, 4, 4, 2), ("z", "y", "x", "c"))
    placed = (
        P(FS, TP),
        P(TP),
        P(FS, TP),
        P(FS, TP),
        P(TP),
        P(TP),
        P(TP, None, None),
        P(TP, None),
        P(TP, FS),
        P(TP),
        P(FS, TP),
        P(FS, TP),
        P(None, TP),
        P(None, TP),
        P(TP, FS),
    )
    return jax.shard_map(on_device, mesh=split, in_specs=placed, out_specs=P(FS, TP), check_vma=False)
```

```python
import jax
import jax.numpy as jnp
from jax import lax
from jax.sharding import Mesh
from jax.sharding import PartitionSpec as P

GROUP_DIM = 128
BLOCK = 128
SEGMENT = 64
KERNEL = 3
SEQ_LEN = 256
FS = ("z", "y")
TP = ("x", "c")
EPS = 1e-06
F32 = jnp.float32
BF16 = jnp.bfloat16
SWAP = [(0, 1), (1, 0)]


def everyones(shard, axis):
    copies = jnp.broadcast_to(shard, (lax.axis_size(axis), *shard.shape))
    return lax.all_to_all(copies, axis, split_axis=0, concat_axis=0, tiled=True)


def other_core(value):
    return lax.ppermute(value, "c", SWAP)


def after(value, *first):
    return lax.optimization_barrier((value, *first))[0]


def by_permutes(shard, axis):
    size = lax.axis_size(axis)
    here = lax.axis_index(axis).astype(jnp.uint32)
    parts = [shard]
    for step in (1, 3, 2):
        parts.append(lax.ppermute(shard, axis, [(i, (i + step) % size) for i in range(size)]))
    filled = jnp.zeros((size, *shard.shape), shard.dtype)
    for step, part in zip((0, 1, 3, 2), parts):
        origin = (here + jnp.uint32(size - step)) & jnp.uint32(size - 1)
        filled = lax.dynamic_update_slice(filled, part[None], (origin, *([jnp.uint32(0)] * shard.ndim)))
    return filled


def matmul(operand, matrix):
    return jnp.dot(operand, matrix, preferred_element_type=F32)


def matmul_t(operand, matrix):
    return lax.dot_general(operand, matrix, (((1,), (1,)), ((), ())), preferred_element_type=F32)


def whole_rows(shard, gather=everyones):
    n, w = shard.shape
    mine = gather(shard, "x")
    other = other_core(mine)
    first = lax.axis_index("c") == 0
    both = jnp.stack([jnp.where(first, mine, other), jnp.where(first, other, mine)], axis=1)
    return both.reshape(-1, n, w).transpose(1, 0, 2).reshape(n, -1)


def rms(values, gain):
    v = values.astype(F32)
    scale = lax.rsqrt(jnp.mean(v * v, axis=1, keepdims=True) + EPS)
    return (v * scale * gain.astype(F32)).astype(BF16)


def causal_taps(values, weights):
    seq_count = values.shape[0] // SEQ_LEN
    shaped = values.reshape(seq_count, SEQ_LEN, values.shape[1])
    padded = jnp.pad(shaped, ((0, 0), (KERNEL - 1, 0), (0, 0)))
    summed = jnp.zeros(shaped.shape, F32)
    for k in range(KERNEL):
        summed = summed + padded[:, k : k + SEQ_LEN].astype(F32) * weights[k].astype(F32)
    return summed.reshape(values.shape[0], values.shape[1])


def product_at_owner(rows, matrix):
    blocks = matrix.reshape(lax.axis_size("x"), 2, -1, matrix.shape[1])
    first = lax.axis_index("c") == 0
    keep = jnp.where(first, blocks[:, 0], blocks[:, 1])
    give = jnp.where(first, blocks[:, 1], blocks[:, 0])
    width = keep.shape[1]

    def split(w):
        return matmul_t(rows, w.reshape(-1, w.shape[2])).astype(BF16)

    came = other_core(split(give))
    pair = (split(keep).astype(F32) + came.astype(F32)).astype(BF16)
    parts = pair.reshape(rows.shape[0], -1, width).transpose(1, 0, 2)
    arrived = lax.all_to_all(parts, "x", split_axis=0, concat_axis=0, tiled=True)
    return arrived.astype(F32).sum(axis=0)


def on_device(
    tokens,
    norm_gain,
    proj_u,
    proj_v,
    layer_gain,
    layer_shift,
    mix_weight,
    mix_bias,
    proj_out,
    ffn_gain,
    ffn_gate,
    ffn_value,
    conv_gate,
    conv_value,
    proj_down,
):
    da = proj_u.shape[1]
    ff = ffn_gate.shape[1]
    row_count = tokens.shape[0]

    early = jnp.concatenate([proj_u, proj_v, proj_out.T], axis=1)
    early_z = everyones(early, "z")
    late = jnp.concatenate([ffn_gate, ffn_value, proj_down.T], axis=1)
    late_y = by_permutes(late, "y").reshape(-1, late.shape[1])
    late_all = lax.all_gather(after(late_y, early_z), "z", axis=0, tiled=True)

    packed = jnp.concatenate([tokens, jnp.broadcast_to(norm_gain, (8, da)), jnp.broadcast_to(ffn_gain, (8, da))], axis=0)
    whole = whole_rows(packed, by_permutes)
    normed = rms(whole[:row_count], whole[row_count])
    gain_two = whole[row_count + 8]
    early_all = everyones(early_z, "y").transpose(1, 0, 2, 3).reshape(-1, early.shape[1])

    act_v = jax.nn.gelu(matmul(normed, early_all[:, da : 2 * da]), approximate=False)
    sums = jnp.stack([jnp.sum(act_v, axis=1), jnp.sum(act_v * act_v, axis=1)])
    totals = everyones(sums.reshape(-1), TP).sum(axis=0).reshape(2, -1)
    act_u = jax.nn.gelu(matmul(normed, early_all[:, :da]), approximate=False)
    full_width = da * lax.axis_size(TP)
    center = totals[0] / full_width
    spread = totals[1] / full_width - center * center
    mixed_in = (
        (act_v - center[:, None]) * lax.rsqrt(spread + EPS)[:, None] * layer_gain.astype(F32) + layer_shift.astype(F32)
    ).astype(BF16)
    groups = da // GROUP_DIM
    blocks = mixed_in.reshape(row_count // BLOCK, BLOCK, groups, GROUP_DIM)
    segment = jnp.arange(BLOCK) // SEGMENT
    visible = segment[None, :] <= segment[:, None]
    masked = jnp.where(visible[None], mix_weight, jnp.zeros_like(mix_weight))
    spatial = (
        jnp.einsum("gij,njgc->nigc", masked, blocks, preferred_element_type=F32)
        + mix_bias.astype(F32).T[None, :, :, None]
    )
    gated = (act_u * spatial.reshape(row_count, da)).astype(BF16)
    stream = (tokens.astype(F32) + product_at_owner(gated, early_all[:, 2 * da :])).astype(BF16)
    normed_two = rms(whole_rows(stream), gain_two)
    pre_gate = matmul(normed_two, late_all[:, :ff]).astype(BF16)
    pre_value = matmul(normed_two, late_all[:, ff : 2 * ff]).astype(BF16)
    conv_g = causal_taps(pre_gate, conv_gate)
    conv_v = causal_taps(pre_value, conv_value)
    hidden = (jax.nn.silu(conv_g) * conv_v).astype(BF16)
    return (stream.astype(F32) + product_at_owner(hidden, late_all[:, 2 * ff :])).astype(BF16)


def solution(mesh):
    split = Mesh(mesh.devices.reshape(16, 4, 4, 2), ("z", "y", "x", "c"))
    placed = (
        P(FS, TP),
        P(TP),
        P(FS, TP),
        P(FS, TP),
        P(TP),
        P(TP),
        P(TP, None, None),
        P(TP, None),
        P(TP, FS),
        P(TP),
        P(FS, TP),
        P(FS, TP),
        P(None, TP),
        P(None, TP),
        P(TP, FS),
    )

    return jax.shard_map(on_device, mesh=split, in_specs=placed, out_specs=P(FS, TP), check_vma=False)
```

```python
import jax
import jax.numpy as jnp
from jax import lax
from jax.experimental import pallas as pl
from jax.experimental.pallas import tpu as pltpu
from jax.sharding import Mesh
from jax.sharding import PartitionSpec as P

GROUP_DIM = 128
BLOCK = 128
SEGMENT = 64
SEQ_LEN = 256
FS = ("z", "y")
TP = ("x", "c")
EPS = 1e-06
F32 = jnp.float32
BF16 = jnp.bfloat16
SWAP = [(0, 1), (1, 0)]
SQRT_HALF = 0.7071067811865476
VMEM = pl.BlockSpec(memory_space=pltpu.VMEM)
SMEM = pl.BlockSpec(memory_space=pltpu.SMEM)


def everyones(shard, axis):
    copies = jnp.broadcast_to(shard, (lax.axis_size(axis), *shard.shape))
    return lax.all_to_all(copies, axis, split_axis=0, concat_axis=0, tiled=True)


def other_core(value):
    return lax.ppermute(value, "c", SWAP)


def after(value, *first):
    return lax.optimization_barrier((value, *first))[0]


def by_permutes(shard, axis):
    size = lax.axis_size(axis)
    here = lax.axis_index(axis).astype(jnp.uint32)
    parts = [shard]
    for step in (1, 3, 2):
        parts.append(lax.ppermute(shard, axis, [(i, (i + step) % size) for i in range(size)]))
    filled = jnp.zeros((size, *shard.shape), shard.dtype)
    for step, part in zip((0, 1, 3, 2), parts):
        origin = (here + jnp.uint32(size - step)) & jnp.uint32(size - 1)
        filled = lax.dynamic_update_slice(filled, part[None], (origin, *([jnp.uint32(0)] * shard.ndim)))
    return filled


def rms(values, gain):
    v = values.astype(F32)
    scale = lax.rsqrt(jnp.mean(v * v, axis=1, keepdims=True) + EPS)
    return (v * scale * gain.astype(F32)).astype(BF16)


def stats_kernel(normed, early, act, sums, weight):
    near = early.shape[0]
    piece = 32
    width = act.shape[1]
    for far in range(early.shape[1] // piece):
        for y in range(near):
            weight[pl.ds((far * near + y) * piece, piece), :] = early[y, pl.ds(far * piece, piece), width : 2 * width]
    for part in range(normed.shape[0] // SEQ_LEN):
        rows = pl.ds(part * SEQ_LEN, SEQ_LEN)
        value = gelu(jnp.dot(normed[rows, :], weight[...], preferred_element_type=F32))
        act[rows, :] = value
        once = sum(value[:, k : k + 128] for k in range(0, width, 128))
        twice = sum(value[:, k : k + 128] * value[:, k : k + 128] for k in range(0, width, 128))
        sums[0:1, rows] = jnp.sum(once.T, axis=0, keepdims=True)
        sums[1:2, rows] = jnp.sum(twice.T, axis=0, keepdims=True)


def gate_kernel(normed, early, act, weight):
    near = early.shape[0]
    piece = 32
    width = act.shape[1]
    for far in range(early.shape[1] // piece):
        for y in range(near):
            weight[pl.ds((far * near + y) * piece, piece), :] = early[y, pl.ds(far * piece, piece), 0:width]
    for part in range(normed.shape[0] // SEQ_LEN):
        rows = pl.ds(part * SEQ_LEN, SEQ_LEN)
        act[rows, :] = gelu(jnp.dot(normed[rows, :], weight[...], preferred_element_type=F32))


def mix_kernel(core, act_v, act_u, stats, gain, shift, mix, bias, early, give, keep, weight, gated):
    near = early.shape[0]
    piece = 32
    width = act_v.shape[1]
    for far in range(early.shape[1] // piece):
        for y in range(near):
            weight[pl.ds((far * near + y) * piece, piece), :] = early[y, pl.ds(far * piece, piece), 2 * width : 3 * width]
    full = width * stats.shape[0]
    i = lax.broadcasted_iota(jnp.int32, (BLOCK, BLOCK), 0)
    j = lax.broadcasted_iota(jnp.int32, (BLOCK, BLOCK), 1)
    visible = (i >= SEGMENT) | (j < SEGMENT)
    total = stats[0]
    for k in range(1, stats.shape[0]):
        total = total + stats[k]
    center_row = total[0:1] / full
    spread_row = total[1:2] / full - center_row * center_row
    scale_row = lax.rsqrt(spread_row + EPS)
    for block in range(act_v.shape[0] // BLOCK):
        rows = pl.ds(block * BLOCK, BLOCK)
        at = slice(block * BLOCK, (block + 1) * BLOCK)
        center = jnp.broadcast_to(center_row[:, at], (BLOCK, BLOCK)).T
        scale = jnp.broadcast_to(scale_row[:, at], (BLOCK, BLOCK)).T
        for g in range(width // GROUP_DIM):
            cols = slice(g * GROUP_DIM, (g + 1) * GROUP_DIM)
            mixed = ((act_v[rows, cols] - center) * scale * gain[:, cols] + shift[:, cols]).astype(BF16)
            seen = jnp.where(visible, mix[g].astype(F32), 0.0).astype(BF16)
            spatial = jnp.dot(seen, mixed, preferred_element_type=F32) + bias[:, g : g + 1]
            gated[rows, cols] = (act_u[rows, cols] * spatial).astype(BF16)
    c = core[0]
    for out, side in ((give, 1 - c), (keep, c)):
        for x in range(out.shape[0]):
            start = pl.multiple_of((2 * x + side) * width, width)
            columns = weight[pl.ds(start, width), :]
            out[x] = lax.dot_general(
                gated[...], columns, (((1,), (1,)), ((), ())), preferred_element_type=F32
            ).astype(BF16)


def shifted(value, by):
    row = lax.broadcasted_iota(jnp.int32, value.shape, 0)
    return jnp.where(row >= by, pltpu.roll(value, by, 0), 0.0)


def taps(value, weights):
    value = value.astype(BF16).astype(F32)
    return (shifted(value, 2) * weights[0:1] + shifted(value, 1) * weights[1:2]) + value * weights[2:3]


def ffn_kernel(core, mine, other, gain, late, conv_gate, conv_value, give, keep, normed, hidden):
    width = mine.shape[2]
    ff = conv_gate.shape[1]
    c = core[0]
    for part in range(mine.shape[1] // SEQ_LEN):
        rows = pl.ds(part * SEQ_LEN, SEQ_LEN)
        squares = jnp.zeros((SEQ_LEN, 1), F32)
        for x in range(mine.shape[0]):
            for ref in (mine, other):
                value = ref[x, rows, :].astype(F32)
                squares = squares + jnp.sum(value * value, axis=1, keepdims=True)
        scale = lax.rsqrt(squares / (2 * mine.shape[0] * width) + EPS)

        def fill(ref, side):
            for x in range(mine.shape[0]):
                at = pl.ds((2 * x + side) * width, width)
                normed[:, at] = (ref[x, rows, :].astype(F32) * scale * gain[:, at]).astype(BF16)

        @pl.when(c == 0)
        def _():
            fill(mine, 0)
            fill(other, 1)

        @pl.when(c == 1)
        def _():
            fill(other, 0)
            fill(mine, 1)

        gate = jnp.dot(normed[...], late[:, 0:ff], preferred_element_type=F32)
        value = jnp.dot(normed[...], late[:, ff : 2 * ff], preferred_element_type=F32)
        conv_g = taps(gate, conv_gate[...])
        conv_v = taps(value, conv_value[...])
        hidden[rows, :] = (conv_g * jax.nn.sigmoid(conv_g) * conv_v).astype(BF16)
    for out, side in ((give, 1 - c), (keep, c)):
        for x in range(out.shape[0]):
            start = pl.multiple_of((2 * x + side) * width, width)
            columns = late[pl.ds(start, width), 2 * ff : 3 * ff]
            out[x] = lax.dot_general(
                hidden[...], columns, (((1,), (1,)), ((), ())), preferred_element_type=F32
            ).astype(BF16)


def gelu(value):
    return 0.5 * value * (1.0 + lax.erf(value * SQRT_HALF))


def shape(dims, dtype):
    return jax.ShapeDtypeStruct(dims, dtype)


def summed_at_owner(give, keep):
    pair = (keep.astype(F32) + other_core(give).astype(F32)).astype(BF16)
    arrived = lax.all_to_all(pair, "x", split_axis=0, concat_axis=0, tiled=True)
    return arrived.astype(F32).sum(axis=0)


def on_device(
    tokens,
    norm_gain,
    proj_u,
    proj_v,
    layer_gain,
    layer_shift,
    mix_weight,
    mix_bias,
    proj_out,
    ffn_gain,
    ffn_gate,
    ffn_value,
    conv_gate,
    conv_value,
    proj_down,
):
    da = proj_u.shape[1]
    ff = ffn_gate.shape[1]
    row_count = tokens.shape[0]

    early = jnp.concatenate([proj_u, proj_v, proj_out.T], axis=1)
    early_z = everyones(early, "z")
    late = jnp.concatenate([ffn_gate, ffn_value, proj_down.T], axis=1)
    late_y = by_permutes(late, "y").reshape(-1, late.shape[1])
    late_all = lax.all_gather(after(late_y, early_z), "z", axis=0, tiled=True)

    packed = jnp.concatenate([tokens, jnp.broadcast_to(norm_gain, (8, da)), jnp.broadcast_to(ffn_gain, (8, da))], axis=0)
    mine = by_permutes(packed, "x")
    other = other_core(mine)
    first = lax.axis_index("c") == 0
    both = jnp.stack([jnp.where(first, mine, other), jnp.where(first, other, mine)], axis=1)
    whole = both.reshape(-1, *packed.shape).transpose(1, 0, 2).reshape(packed.shape[0], -1)
    normed = rms(whole[:row_count], whole[row_count])
    gain_two = whole[row_count + 8]
    early_all = everyones(early_z, "y").reshape(4, -1, early.shape[1])
    core = lax.axis_index("c").astype(jnp.int32).reshape(1)
    model = proj_u.shape[0] * lax.axis_size(FS)

    act_v, sums = pl.pallas_call(
        stats_kernel,
        in_specs=[VMEM] * 2,
        out_specs=[VMEM] * 2,
        out_shape=[shape((row_count, da), F32), shape((2, row_count), F32)],
        scratch_shapes=[pltpu.VMEM((model, da), BF16)],
        name="stats",
    )(normed, early_all)
    stats = everyones(sums, TP)
    act_u = pl.pallas_call(
        gate_kernel,
        in_specs=[VMEM] * 2,
        out_specs=VMEM,
        out_shape=shape((row_count, da), F32),
        scratch_shapes=[pltpu.VMEM((model, da), BF16)],
        name="gate",
    )(normed, early_all)
    blocks = [shape((lax.axis_size("x"), row_count, da), BF16)] * 2
    give, keep = pl.pallas_call(
        mix_kernel,
        in_specs=[SMEM] + [VMEM] * 8,
        out_specs=[VMEM] * 2,
        out_shape=blocks,
        scratch_shapes=[pltpu.VMEM((model, da), BF16), pltpu.VMEM((row_count, da), BF16)],
        name="mix",
    )(
        core,
        act_v,
        act_u,
        stats,
        layer_gain.astype(F32)[None],
        layer_shift.astype(F32)[None],
        mix_weight,
        mix_bias.astype(F32).T,
        early_all,
    )
    stream = (tokens.astype(F32) + summed_at_owner(give, keep)).astype(BF16)
    mine = everyones(stream, "x")
    give, keep = pl.pallas_call(
        ffn_kernel,
        in_specs=[SMEM] + [VMEM] * 6,
        out_specs=[VMEM] * 2,
        out_shape=blocks,
        scratch_shapes=[pltpu.VMEM((SEQ_LEN, model), BF16), pltpu.VMEM((row_count, ff), BF16)],
        name="ffn",
    )(
        core,
        mine,
        other_core(mine),
        gain_two.astype(F32)[None],
        late_all,
        conv_gate.astype(F32),
        conv_value.astype(F32),
    )
    return (stream.astype(F32) + summed_at_owner(give, keep)).astype(BF16)


def solution(mesh):
    split = Mesh(mesh.devices.reshape(16, 4, 4, 2), ("z", "y", "x", "c"))
    placed = (
        P(FS, TP),
        P(TP),
        P(FS, TP),
        P(FS, TP),
        P(TP),
        P(TP),
        P(TP, None, None),
        P(TP, None),
        P(TP, FS),
        P(TP),
        P(FS, TP),
        P(FS, TP),
        P(None, TP),
        P(None, TP),
        P(TP, FS),
    )

    return jax.shard_map(on_device, mesh=split, in_specs=placed, out_specs=P(FS, TP), check_vma=False)
```

```python
import jax
import jax.numpy as jnp
from jax import lax
from jax.experimental import pallas as pl
from jax.experimental.pallas import tpu as pltpu
from jax.sharding import Mesh
from jax.sharding import PartitionSpec as P

GROUP_DIM = 128
BLOCK = 128
SEGMENT = 64
SEQ_LEN = 256
FS = ("z", "y")
TP = ("x", "c")
EPS = 1e-06
F32 = jnp.float32
BF16 = jnp.bfloat16
SWAP = [(0, 1), (1, 0)]
RING = (0, 1, 3, 2)
SQRT_HALF = 0.7071067811865476
VMEM = pl.BlockSpec(memory_space=pltpu.VMEM)
SMEM = pl.BlockSpec(memory_space=pltpu.SMEM)


def everyones(shard, axis):
    copies = jnp.broadcast_to(shard, (lax.axis_size(axis), *shard.shape))
    return lax.all_to_all(copies, axis, split_axis=0, concat_axis=0, tiled=True)


def other_core(value):
    return lax.ppermute(value, "c", SWAP)


def after(value, *first):
    return lax.optimization_barrier((value, *first))[0]


def round_ring(shard, axis):
    return [shard] + [lax.ppermute(shard, axis, [(i, (i + step) % 4) for i in range(4)]) for step in RING[1:]]


def in_order(parts, axis):
    here = lax.axis_index(axis).astype(jnp.uint32)
    filled = jnp.zeros((4, *parts[0].shape), parts[0].dtype)
    for step, part in zip(RING, parts):
        at = (here + jnp.uint32(4 - step)) & jnp.uint32(3)
        filled = lax.dynamic_update_slice(filled, part[None], (at, *([jnp.uint32(0)] * part.ndim)))
    return filled


def norm_kernel(place, *refs):
    parts, (out, gain_two) = refs[:8], refs[8:]
    count, width = parts[0].shape[0] - 16, parts[0].shape[1]
    x, c = place[0], place[1]
    for part in range(count // BLOCK):
        rows = pl.ds(part * BLOCK, BLOCK)
        squares = jnp.zeros((BLOCK, width), F32)
        for ref in parts:
            value = ref[rows, :].astype(F32)
            squares = squares + value * value
        scale = lax.rsqrt(jnp.sum(squares, axis=1, keepdims=True) / (8 * width) + EPS)
        for at, ref in enumerate(parts):
            block = origin(x, RING[at % 4]) * 2 + (c if at < 4 else 1 - c)
            gain = ref[count : count + 1, :].astype(F32)
            out[rows, pl.ds(pl.multiple_of(block * width, width), width)] = (
                ref[rows, :].astype(F32) * scale * gain
            ).astype(BF16)
    for at, ref in enumerate(parts):
        block = origin(x, RING[at % 4]) * 2 + (c if at < 4 else 1 - c)
        gain_two[block] = ref[count + 8 : count + 16, :]


def origin(here, step):
    return (here + (4 - step)) & 3


def stats_kernel(normed, early, act, sums, weight):
    near = early.shape[0]
    piece = 32
    width = act.shape[1]
    for far in range(early.shape[1] // piece):
        for y in range(near):
            weight[pl.ds((far * near + y) * piece, piece), :] = early[y, pl.ds(far * piece, piece), width : 2 * width]
    for part in range(normed.shape[0] // SEQ_LEN):
        rows = pl.ds(part * SEQ_LEN, SEQ_LEN)
        value = gelu(jnp.dot(normed[rows, :], weight[...], preferred_element_type=F32))
        act[rows, :] = value
        once = sum(value[:, k : k + 128] for k in range(0, width, 128))
        twice = sum(value[:, k : k + 128] * value[:, k : k + 128] for k in range(0, width, 128))
        sums[0:1, rows] = jnp.sum(once.T, axis=0, keepdims=True)
        sums[1:2, rows] = jnp.sum(twice.T, axis=0, keepdims=True)


def gate_kernel(normed, early, act, weight):
    near = early.shape[0]
    piece = 32
    width = act.shape[1]
    for far in range(early.shape[1] // piece):
        for y in range(near):
            weight[pl.ds((far * near + y) * piece, piece), :] = early[y, pl.ds(far * piece, piece), 0:width]
    for part in range(normed.shape[0] // SEQ_LEN):
        rows = pl.ds(part * SEQ_LEN, SEQ_LEN)
        act[rows, :] = gelu(jnp.dot(normed[rows, :], weight[...], preferred_element_type=F32))


def mix_kernel(core, act_v, act_u, stats, gain, shift, mix, bias, early, give, keep, weight, gated):
    near = early.shape[0]
    piece = 32
    width = act_v.shape[1]
    for far in range(early.shape[1] // piece):
        for y in range(near):
            weight[pl.ds((far * near + y) * piece, piece), :] = early[y, pl.ds(far * piece, piece), 2 * width : 3 * width]
    full = width * stats.shape[0]
    i = lax.broadcasted_iota(jnp.int32, (BLOCK, BLOCK), 0)
    j = lax.broadcasted_iota(jnp.int32, (BLOCK, BLOCK), 1)
    visible = (i >= SEGMENT) | (j < SEGMENT)
    total = stats[0]
    for k in range(1, stats.shape[0]):
        total = total + stats[k]
    center_row = total[0:1] / full
    spread_row = total[1:2] / full - center_row * center_row
    scale_row = lax.rsqrt(spread_row + EPS)
    biases = [jnp.broadcast_to(bias[g : g + 1, :].astype(F32), (BLOCK, BLOCK)).T for g in range(width // GROUP_DIM)]
    for block in range(act_v.shape[0] // BLOCK):
        rows = pl.ds(block * BLOCK, BLOCK)
        at = slice(block * BLOCK, (block + 1) * BLOCK)
        center = jnp.broadcast_to(center_row[:, at], (BLOCK, BLOCK)).T
        scale = jnp.broadcast_to(scale_row[:, at], (BLOCK, BLOCK)).T
        for g in range(width // GROUP_DIM):
            cols = slice(g * GROUP_DIM, (g + 1) * GROUP_DIM)
            mixed = ((act_v[rows, cols] - center) * scale * gain[:, cols].astype(F32) + shift[:, cols].astype(F32)).astype(BF16)
            seen = jnp.where(visible, mix[g].astype(F32), 0.0).astype(BF16)
            spatial = jnp.dot(seen, mixed, preferred_element_type=F32) + biases[g]
            gated[rows, cols] = (act_u[rows, cols] * spatial).astype(BF16)
    c = core[0]
    for out, side in ((give, 1 - c), (keep, c)):
        for x in range(out.shape[0]):
            start = pl.multiple_of((2 * x + side) * width, width)
            columns = weight[pl.ds(start, width), :]
            out[x] = lax.dot_general(
                gated[...], columns, (((1,), (1,)), ((), ())), preferred_element_type=F32
            ).astype(BF16)


def shifted(value, by):
    row = lax.broadcasted_iota(jnp.int32, value.shape, 0)
    return jnp.where(row >= by, pltpu.roll(value, by, 0), 0.0)


def taps(value, weights):
    value = value.astype(BF16).astype(F32)
    return (shifted(value, 2) * weights[0:1] + shifted(value, 1) * weights[1:2]) + value * weights[2:3]


def ffn_kernel(core, mine, other, gain, late, conv_gate, conv_value, give, keep, normed, hidden):
    width = mine.shape[2]
    ff = conv_gate.shape[1]
    c = core[0]
    for part in range(mine.shape[1] // SEQ_LEN):
        rows = pl.ds(part * SEQ_LEN, SEQ_LEN)
        squares = jnp.zeros((SEQ_LEN, 1), F32)
        for x in range(mine.shape[0]):
            for ref in (mine, other):
                value = ref[x, rows, :].astype(F32)
                squares = squares + jnp.sum(value * value, axis=1, keepdims=True)
        scale = lax.rsqrt(squares / (2 * mine.shape[0] * width) + EPS)

        def fill(ref, side):
            for x in range(mine.shape[0]):
                at = pl.ds((2 * x + side) * width, width)
                row = gain[2 * x + side, 0:1, :].astype(F32)
                normed[:, at] = (ref[x, rows, :].astype(F32) * scale * row).astype(BF16)

        @pl.when(c == 0)
        def _():
            fill(mine, 0)
            fill(other, 1)

        @pl.when(c == 1)
        def _():
            fill(other, 0)
            fill(mine, 1)

        gate = jnp.dot(normed[...], late[:, 0:ff], preferred_element_type=F32)
        value = jnp.dot(normed[...], late[:, ff : 2 * ff], preferred_element_type=F32)
        conv_g = taps(gate, conv_gate[...].astype(F32))
        conv_v = taps(value, conv_value[...].astype(F32))
        hidden[rows, :] = (conv_g * jax.nn.sigmoid(conv_g) * conv_v).astype(BF16)
    for out, side in ((give, 1 - c), (keep, c)):
        for x in range(out.shape[0]):
            start = pl.multiple_of((2 * x + side) * width, width)
            columns = late[pl.ds(start, width), 2 * ff : 3 * ff]
            out[x] = lax.dot_general(
                hidden[...], columns, (((1,), (1,)), ((), ())), preferred_element_type=F32
            ).astype(BF16)


def gelu(value):
    return 0.5 * value * (1.0 + lax.erf(value * SQRT_HALF))


def shape(dims, dtype):
    return jax.ShapeDtypeStruct(dims, dtype)


def room(mebibytes):
    return pltpu.CompilerParams(vmem_limit_bytes=mebibytes << 20)


def summed_at_owner(give, keep):
    pair = (keep.astype(F32) + other_core(give).astype(F32)).astype(BF16)
    arrived = lax.all_to_all(pair, "x", split_axis=0, concat_axis=0, tiled=True)
    return arrived.astype(F32).sum(axis=0)


def on_device(
    tokens,
    norm_gain,
    proj_u,
    proj_v,
    layer_gain,
    layer_shift,
    mix_weight,
    mix_bias,
    proj_out,
    ffn_gain,
    ffn_gate,
    ffn_value,
    conv_gate,
    conv_value,
    proj_down,
):
    da = proj_u.shape[1]
    ff = ffn_gate.shape[1]
    row_count = tokens.shape[0]

    early = jnp.concatenate([proj_u, proj_v, proj_out.T], axis=1)
    early_z = everyones(early, "z")
    late = jnp.concatenate([ffn_gate, ffn_value, proj_down.T], axis=1)
    late_y = in_order(round_ring(late, "y"), "y").reshape(-1, late.shape[1])
    late_all = lax.all_gather(after(late_y, early_z), "z", axis=0, tiled=True)

    packed = jnp.concatenate([tokens, jnp.broadcast_to(norm_gain, (8, da)), jnp.broadcast_to(ffn_gain, (8, da))], axis=0)
    mine = round_ring(packed, "x")
    other = [other_core(part) for part in mine]
    early_all = everyones(early_z, "y").reshape(4, -1, early.shape[1])
    core = lax.axis_index("c").astype(jnp.int32)
    place = jnp.stack([lax.axis_index("x").astype(jnp.int32), core])
    core = core.reshape(1)
    model = proj_u.shape[0] * lax.axis_size(FS)
    tp = lax.axis_size(TP)
    normed, gain_two = pl.pallas_call(
        norm_kernel,
        in_specs=[SMEM] + [VMEM] * 8,
        out_specs=[VMEM] * 2,
        out_shape=[shape((row_count, model), BF16), shape((tp, 8, da), BF16)],
        name="norm",
        compiler_params=room(12),
    )(place, *mine, *other)

    act_v, sums = pl.pallas_call(
        stats_kernel,
        in_specs=[VMEM] * 2,
        out_specs=[VMEM] * 2,
        out_shape=[shape((row_count, da), F32), shape((2, row_count), F32)],
        scratch_shapes=[pltpu.VMEM((model, da), BF16)],
        name="stats",
        compiler_params=room(14),
    )(normed, early_all)
    stats = everyones(sums, TP)
    act_u = pl.pallas_call(
        gate_kernel,
        in_specs=[VMEM] * 2,
        out_specs=VMEM,
        out_shape=shape((row_count, da), F32),
        scratch_shapes=[pltpu.VMEM((model, da), BF16)],
        name="gate",
        compiler_params=room(14),
    )(normed, early_all)
    blocks = [shape((lax.axis_size("x"), row_count, da), BF16)] * 2
    give, keep = pl.pallas_call(
        mix_kernel,
        in_specs=[SMEM] + [VMEM] * 8,
        out_specs=[VMEM] * 2,
        out_shape=blocks,
        scratch_shapes=[pltpu.VMEM((model, da), BF16), pltpu.VMEM((row_count, da), BF16)],
        name="mix",
        compiler_params=room(16),
    )(
        core,
        act_v,
        act_u,
        stats,
        layer_gain[None],
        layer_shift[None],
        mix_weight,
        mix_bias,
        early_all,
    )
    stream = (tokens.astype(F32) + summed_at_owner(give, keep)).astype(BF16)
    mine = everyones(stream, "x")
    give, keep = pl.pallas_call(
        ffn_kernel,
        in_specs=[SMEM] + [VMEM] * 6,
        out_specs=[VMEM] * 2,
        out_shape=blocks,
        scratch_shapes=[pltpu.VMEM((SEQ_LEN, model), BF16), pltpu.VMEM((row_count, ff), BF16)],
        name="ffn",
        compiler_params=room(26),
    )(
        core,
        mine,
        other_core(mine),
        gain_two,
        late_all,
        conv_gate,
        conv_value,
    )
    return (stream.astype(F32) + summed_at_owner(give, keep)).astype(BF16)


def solution(mesh):
    split = Mesh(mesh.devices.reshape(16, 4, 4, 2), ("z", "y", "x", "c"))
    placed = (
        P(FS, TP),
        P(TP),
        P(FS, TP),
        P(FS, TP),
        P(TP),
        P(TP),
        P(TP, None, None),
        P(TP, None),
        P(TP, FS),
        P(TP),
        P(FS, TP),
        P(FS, TP),
        P(None, TP),
        P(None, TP),
        P(TP, FS),
    )

    return jax.shard_map(on_device, mesh=split, in_specs=placed, out_specs=P(FS, TP), check_vma=False)
```

```python
import jax
import jax.numpy as jnp
from jax import lax
from jax.experimental import pallas as pl
from jax.experimental.pallas import tpu as pltpu
from jax.sharding import Mesh
from jax.sharding import PartitionSpec as P

GROUP_DIM = 128
BLOCK = 128
SEGMENT = 64
SEQ_LEN = 256
FS = ("z", "y")
TP = ("x", "c")
EPS = 1e-06
F32 = jnp.float32
BF16 = jnp.bfloat16
SWAP = [(0, 1), (1, 0)]
RING = (0, 1, 3, 2)
PIECE = 32
ANY = pl.BlockSpec(memory_space=pl.ANY)
SQRT_HALF = 0.7071067811865476
VMEM = pl.BlockSpec(memory_space=pltpu.VMEM)
SMEM = pl.BlockSpec(memory_space=pltpu.SMEM)


def everyones(shard, axis):
    copies = jnp.broadcast_to(shard, (lax.axis_size(axis), *shard.shape))
    return lax.all_to_all(copies, axis, split_axis=0, concat_axis=0, tiled=True)


def other_core(value):
    return lax.ppermute(value, "c", SWAP)


def after(value, *first):
    return lax.optimization_barrier((value, *first))[0]


def round_ring(shard, axis):
    return [shard] + [lax.ppermute(shard, axis, [(i, (i + step) % 4) for i in range(4)]) for step in RING[1:]]


def in_order(parts, axis):
    here = lax.axis_index(axis).astype(jnp.uint32)
    filled = jnp.zeros((4, *parts[0].shape), parts[0].dtype)
    for step, part in zip(RING, parts):
        at = (here + jnp.uint32(4 - step)) & jnp.uint32(3)
        filled = lax.dynamic_update_slice(filled, part[None], (at, *([jnp.uint32(0)] * part.ndim)))
    return filled


def norm_kernel(place, *refs):
    parts, (out, gain_two) = refs[:8], refs[8:]
    count, width = parts[0].shape[0] - 16, parts[0].shape[1]
    x, c = place[0], place[1]
    for part in range(count // BLOCK):
        rows = pl.ds(part * BLOCK, BLOCK)
        squares = jnp.zeros((BLOCK, width), F32)
        for ref in parts:
            value = ref[rows, :].astype(F32)
            squares = squares + value * value
        scale = lax.rsqrt(jnp.sum(squares, axis=1, keepdims=True) / (8 * width) + EPS)
        for at, ref in enumerate(parts):
            block = origin(x, RING[at % 4]) * 2 + (c if at < 4 else 1 - c)
            gain = ref[count : count + 1, :].astype(F32)
            out[rows, pl.ds(pl.multiple_of(block * width, width), width)] = (
                ref[rows, :].astype(F32) * scale * gain
            ).astype(BF16)
    for at, ref in enumerate(parts):
        block = origin(x, RING[at % 4]) * 2 + (c if at < 4 else 1 - c)
        gain_two[block] = ref[count + 8 : count + 16, :]


def origin(here, step):
    return (here + (4 - step)) & 3


def fill_rows(weight, parts, y, cols):
    for step, part in zip(RING, parts):
        near = origin(y, step)
        for far in range(part.shape[0] // PIECE):
            start = pl.multiple_of((far * 4 + near) * PIECE, PIECE)
            weight[pl.ds(start, PIECE), :] = part[far * PIECE : (far + 1) * PIECE, cols]


def stats_kernel(place, normed, p0, p1, p2, p3, act, sums, weight):
    width = act.shape[1]
    fill_rows(weight, (p0, p1, p2, p3), place[2], slice(width, 2 * width))
    for part in range(normed.shape[0] // SEQ_LEN):
        rows = pl.ds(part * SEQ_LEN, SEQ_LEN)
        value = gelu(jnp.dot(normed[rows, :], weight[...], preferred_element_type=F32))
        act[rows, :] = value
        once = sum(value[:, k : k + 128] for k in range(0, width, 128))
        twice = sum(value[:, k : k + 128] * value[:, k : k + 128] for k in range(0, width, 128))
        sums[0:1, rows] = jnp.sum(once.T, axis=0, keepdims=True)
        sums[1:2, rows] = jnp.sum(twice.T, axis=0, keepdims=True)


def gate_kernel(place, normed, p0, p1, p2, p3, act, weight):
    fill_rows(weight, (p0, p1, p2, p3), place[2], slice(0, act.shape[1]))
    for part in range(normed.shape[0] // SEQ_LEN):
        rows = pl.ds(part * SEQ_LEN, SEQ_LEN)
        act[rows, :] = gelu(jnp.dot(normed[rows, :], weight[...], preferred_element_type=F32))


def mix_kernel(place, act_v, act_u, stats, gain, shift, mix, bias, p0, p1, p2, p3, give, keep, weight, gated):
    width = act_v.shape[1]
    fill_rows(weight, (p0, p1, p2, p3), place[2], slice(0, width))
    full = width * stats.shape[0]
    i = lax.broadcasted_iota(jnp.int32, (BLOCK, BLOCK), 0)
    j = lax.broadcasted_iota(jnp.int32, (BLOCK, BLOCK), 1)
    visible = (i >= SEGMENT) | (j < SEGMENT)
    total = stats[0]
    for k in range(1, stats.shape[0]):
        total = total + stats[k]
    center_row = total[0:1] / full
    spread_row = total[1:2] / full - center_row * center_row
    scale_row = lax.rsqrt(spread_row + EPS)
    biases = [jnp.broadcast_to(bias[g : g + 1, :].astype(F32), (BLOCK, BLOCK)).T for g in range(width // GROUP_DIM)]
    for block in range(act_v.shape[0] // BLOCK):
        rows = pl.ds(block * BLOCK, BLOCK)
        at = slice(block * BLOCK, (block + 1) * BLOCK)
        center = jnp.broadcast_to(center_row[:, at], (BLOCK, BLOCK)).T
        scale = jnp.broadcast_to(scale_row[:, at], (BLOCK, BLOCK)).T
        for g in range(width // GROUP_DIM):
            cols = slice(g * GROUP_DIM, (g + 1) * GROUP_DIM)
            mixed = ((act_v[rows, cols] - center) * scale * gain[:, cols].astype(F32) + shift[:, cols].astype(F32)).astype(BF16)
            seen = jnp.where(visible, mix[g].astype(F32), 0.0).astype(BF16)
            spatial = jnp.dot(seen, mixed, preferred_element_type=F32) + biases[g]
            gated[rows, cols] = (act_u[rows, cols] * spatial).astype(BF16)
    c = place[1]
    for out, side in ((give, 1 - c), (keep, c)):
        for x in range(out.shape[0]):
            start = pl.multiple_of((2 * x + side) * width, width)
            columns = weight[pl.ds(start, width), :]
            out[x] = lax.dot_general(
                gated[...], columns, (((1,), (1,)), ((), ())), preferred_element_type=F32
            ).astype(BF16)


def shifted(value, by):
    row = lax.broadcasted_iota(jnp.int32, value.shape, 0)
    return jnp.where(row >= by, pltpu.roll(value, by, 0), 0.0)


def taps(value, weights):
    value = value.astype(BF16).astype(F32)
    return (shifted(value, 2) * weights[0:1] + shifted(value, 1) * weights[1:2]) + value * weights[2:3]


def ffn_kernel(place, mine, other, gain, late_hbm, conv_gate, conv_value, give, keep, normed, hidden, late, done):
    width = mine.shape[2]
    ff = conv_gate.shape[1]
    c = place[1]
    copies = [
        pltpu.make_async_copy(late_hbm.at[:, pl.ds(k * ff, ff)], late.at[:, pl.ds(k * ff, ff)], done.at[k])
        for k in range(3)
    ]
    for copy in copies:
        copy.start()
    for part in range(mine.shape[1] // SEQ_LEN):
        rows = pl.ds(part * SEQ_LEN, SEQ_LEN)
        squares = jnp.zeros((SEQ_LEN, 1), F32)
        for x in range(mine.shape[0]):
            for ref in (mine, other):
                value = ref[x, rows, :].astype(F32)
                squares = squares + jnp.sum(value * value, axis=1, keepdims=True)
        scale = lax.rsqrt(squares / (2 * mine.shape[0] * width) + EPS)

        def fill(ref, side):
            for x in range(mine.shape[0]):
                at = pl.ds((2 * x + side) * width, width)
                row = gain[2 * x + side, 0:1, :].astype(F32)
                normed[:, at] = (ref[x, rows, :].astype(F32) * scale * row).astype(BF16)

        @pl.when(c == 0)
        def _():
            fill(mine, 0)
            fill(other, 1)

        @pl.when(c == 1)
        def _():
            fill(other, 0)
            fill(mine, 1)

        if part == 0:
            copies[0].wait()
        gate = jnp.dot(normed[...], late[:, 0:ff], preferred_element_type=F32)
        if part == 0:
            copies[1].wait()
        value = jnp.dot(normed[...], late[:, ff : 2 * ff], preferred_element_type=F32)
        conv_g = taps(gate, conv_gate[...].astype(F32))
        conv_v = taps(value, conv_value[...].astype(F32))
        hidden[rows, :] = (conv_g * jax.nn.sigmoid(conv_g) * conv_v).astype(BF16)
    copies[2].wait()
    for out, side in ((give, 1 - c), (keep, c)):
        for x in range(out.shape[0]):
            start = pl.multiple_of((2 * x + side) * width, width)
            columns = late[pl.ds(start, width), 2 * ff : 3 * ff]
            out[x] = lax.dot_general(
                hidden[...], columns, (((1,), (1,)), ((), ())), preferred_element_type=F32
            ).astype(BF16)


def gelu(value):
    return 0.5 * value * (1.0 + lax.erf(value * SQRT_HALF))


def shape(dims, dtype):
    return jax.ShapeDtypeStruct(dims, dtype)


def room(mebibytes):
    return pltpu.CompilerParams(vmem_limit_bytes=mebibytes << 20)


def summed_at_owner(give, keep):
    pair = (keep.astype(F32) + other_core(give).astype(F32)).astype(BF16)
    arrived = lax.all_to_all(pair, "x", split_axis=0, concat_axis=0, tiled=True)
    return arrived.astype(F32).sum(axis=0)


def on_device(
    tokens,
    norm_gain,
    proj_u,
    proj_v,
    layer_gain,
    layer_shift,
    mix_weight,
    mix_bias,
    proj_out,
    ffn_gain,
    ffn_gate,
    ffn_value,
    conv_gate,
    conv_value,
    proj_down,
):
    da = proj_u.shape[1]
    ff = ffn_gate.shape[1]
    row_count = tokens.shape[0]

    early = jnp.concatenate([proj_u, proj_v], axis=1)
    early_z = everyones(early, "z").reshape(-1, early.shape[1])
    late = jnp.concatenate([ffn_gate, ffn_value, proj_down.T], axis=1)
    late_y = in_order(round_ring(late, "y"), "y").reshape(-1, late.shape[1])
    late_all = lax.all_gather(after(late_y, early_z), "z", axis=0, tiled=True)

    packed = jnp.concatenate([tokens, jnp.broadcast_to(norm_gain, (8, da)), jnp.broadcast_to(ffn_gain, (8, da))], axis=0)
    mine = round_ring(packed, "x")
    early_parts = round_ring(early_z, "y")
    out_z = everyones(proj_out.T, "z").reshape(-1, da)
    other = [other_core(part) for part in mine]
    out_parts = round_ring(out_z, "y")
    place = jnp.stack([lax.axis_index(name).astype(jnp.int32) for name in ("x", "c", "y")])
    model = proj_u.shape[0] * lax.axis_size(FS)
    tp = lax.axis_size(TP)
    normed, gain_two = pl.pallas_call(
        norm_kernel,
        in_specs=[SMEM] + [VMEM] * 8,
        out_specs=[VMEM] * 2,
        out_shape=[shape((row_count, model), BF16), shape((tp, 8, da), BF16)],
        name="norm",
        compiler_params=room(12),
    )(place, *mine, *other)

    act_v, sums = pl.pallas_call(
        stats_kernel,
        in_specs=[SMEM] + [VMEM] * 5,
        out_specs=[VMEM] * 2,
        out_shape=[shape((row_count, da), F32), shape((2, row_count), F32)],
        scratch_shapes=[pltpu.VMEM((model, da), BF16)],
        name="stats",
        compiler_params=room(14),
    )(place, normed, *early_parts)
    stats = everyones(sums, TP)
    act_u = pl.pallas_call(
        gate_kernel,
        in_specs=[SMEM] + [VMEM] * 5,
        out_specs=VMEM,
        out_shape=shape((row_count, da), F32),
        scratch_shapes=[pltpu.VMEM((model, da), BF16)],
        name="gate",
        compiler_params=room(14),
    )(place, normed, *early_parts)
    blocks = [shape((lax.axis_size("x"), row_count, da), BF16)] * 2
    give, keep = pl.pallas_call(
        mix_kernel,
        in_specs=[SMEM] + [VMEM] * 11,
        out_specs=[VMEM] * 2,
        out_shape=blocks,
        scratch_shapes=[pltpu.VMEM((model, da), BF16), pltpu.VMEM((row_count, da), BF16)],
        name="mix",
        compiler_params=room(16),
    )(
        place,
        act_v,
        act_u,
        stats,
        layer_gain[None],
        layer_shift[None],
        mix_weight,
        mix_bias,
        *out_parts,
    )
    stream = (tokens.astype(F32) + summed_at_owner(give, keep)).astype(BF16)
    mine = everyones(stream, "x")
    give, keep = pl.pallas_call(
        ffn_kernel,
        in_specs=[SMEM] + [VMEM] * 3 + [ANY] + [VMEM] * 2,
        out_specs=[VMEM] * 2,
        out_shape=blocks,
        scratch_shapes=[pltpu.VMEM((SEQ_LEN, model), BF16), pltpu.VMEM((row_count, ff), BF16), pltpu.VMEM(late_all.shape, BF16), pltpu.SemaphoreType.DMA((3,))],
        name="ffn",
        compiler_params=room(26),
    )(
        place,
        mine,
        other_core(mine),
        gain_two,
        late_all,
        conv_gate,
        conv_value,
    )
    return (stream.astype(F32) + summed_at_owner(give, keep)).astype(BF16)


def solution(mesh):
    split = Mesh(mesh.devices.reshape(16, 4, 4, 2), ("z", "y", "x", "c"))
    placed = (
        P(FS, TP),
        P(TP),
        P(FS, TP),
        P(FS, TP),
        P(TP),
        P(TP),
        P(TP, None, None),
        P(TP, None),
        P(TP, FS),
        P(TP),
        P(FS, TP),
        P(FS, TP),
        P(None, TP),
        P(None, TP),
        P(TP, FS),
    )

    return jax.shard_map(on_device, mesh=split, in_specs=placed, out_specs=P(FS, TP), check_vma=False)
```

```python
import jax
import jax.numpy as jnp
from jax import lax
from jax.experimental import pallas as pl
from jax.experimental.pallas import tpu as pltpu
from jax.sharding import Mesh
from jax.sharding import PartitionSpec as P

GROUP_DIM = 128
BLOCK = 128
SEGMENT = 64
SEQ_LEN = 256
Z = ("zh", "zl")
FS = ("zh", "zl", "y")
TP = ("x", "c")
EPS = 1e-06
F32 = jnp.float32
BF16 = jnp.bfloat16
SWAP = [(0, 1), (1, 0)]
RING = (0, 1, 3, 2)
PIECE = 32
HBM = pl.BlockSpec(memory_space=pltpu.HBM)
SQRT_HALF = 0.7071067811865476
VMEM = pl.BlockSpec(memory_space=pltpu.VMEM)
SMEM = pl.BlockSpec(memory_space=pltpu.SMEM)


def everyones(shard, axis):
    copies = jnp.broadcast_to(shard, (lax.axis_size(axis), *shard.shape))
    return lax.all_to_all(copies, axis, split_axis=0, concat_axis=0, tiled=True)


def other_core(value):
    return lax.ppermute(value, "c", SWAP)


def after(value, *first):
    return lax.optimization_barrier((value, *first))[0]


def round_ring(shard, axis):
    size = lax.axis_size(axis)
    steps = (1, size - 1, 2)
    return [shard] + [lax.ppermute(shard, axis, [(i, (i + step) % size) for i in range(size)]) for step in steps]


def in_order(parts, axis):
    here = lax.axis_index(axis).astype(jnp.uint32)
    filled = jnp.zeros((4, *parts[0].shape), parts[0].dtype)
    for step, part in zip(RING, parts):
        at = (here + jnp.uint32(4 - step)) & jnp.uint32(3)
        filled = lax.dynamic_update_slice(filled, part[None], (at, *([jnp.uint32(0)] * part.ndim)))
    return filled


def norm_kernel(place, *refs):
    parts, (out, gain_two) = refs[:8], refs[8:]
    count, width = parts[0].shape[0] - 16, parts[0].shape[1]
    x, c = place[0], place[1]
    for part in range(count // BLOCK):
        rows = pl.ds(part * BLOCK, BLOCK)
        squares = jnp.zeros((BLOCK, width), F32)
        for ref in parts:
            value = ref[rows, :].astype(F32)
            squares = squares + value * value
        scale = lax.rsqrt(jnp.sum(squares, axis=1, keepdims=True) / (8 * width) + EPS)
        for at, ref in enumerate(parts):
            block = origin(x, RING[at % 4]) * 2 + (c if at < 4 else 1 - c)
            gain = ref[count : count + 1, :].astype(F32)
            out[rows, pl.ds(pl.multiple_of(block * width, width), width)] = (
                ref[rows, :].astype(F32) * scale * gain
            ).astype(BF16)
    for at, ref in enumerate(parts):
        block = origin(x, RING[at % 4]) * 2 + (c if at < 4 else 1 - c)
        gain_two[block] = ref[count + 8 : count + 16, :]


def origin(here, step):
    return (here + (4 - step)) & 3


def fill_rows(weight, early, near, cols):
    for y in range(4):
        for at, step in enumerate(RING):
            for far in range(4):
                start = pl.multiple_of(((far * 4 + origin(near, step)) * 4 + y) * PIECE, PIECE)
                came = (at * 4 + far) * PIECE
                weight[pl.ds(start, PIECE), :] = early[y, came : came + PIECE, cols]


def stats_kernel(place, normed, early, act, sums, weight):
    width = act.shape[1]
    fill_rows(weight, early, place[2], slice(width, 2 * width))
    for part in range(normed.shape[0] // SEQ_LEN):
        rows = pl.ds(part * SEQ_LEN, SEQ_LEN)
        value = gelu(jnp.dot(normed[rows, :], weight[...], preferred_element_type=F32))
        act[rows, :] = value
        once = sum(value[:, k : k + 128] for k in range(0, width, 128))
        twice = sum(value[:, k : k + 128] * value[:, k : k + 128] for k in range(0, width, 128))
        sums[0:1, rows] = jnp.sum(once.T, axis=0, keepdims=True)
        sums[1:2, rows] = jnp.sum(twice.T, axis=0, keepdims=True)


def gate_kernel(place, normed, early, act, weight):
    fill_rows(weight, early, place[2], slice(0, act.shape[1]))
    for part in range(normed.shape[0] // SEQ_LEN):
        rows = pl.ds(part * SEQ_LEN, SEQ_LEN)
        act[rows, :] = gelu(jnp.dot(normed[rows, :], weight[...], preferred_element_type=F32))


def mix_kernel(place, act_v, act_u, stats, gain, shift, mix, bias, early, give, keep, weight, gated):
    width = act_v.shape[1]
    fill_rows(weight, early, place[2], slice(2 * width, 3 * width))
    full = width * stats.shape[0]
    i = lax.broadcasted_iota(jnp.int32, (BLOCK, BLOCK), 0)
    j = lax.broadcasted_iota(jnp.int32, (BLOCK, BLOCK), 1)
    visible = (i >= SEGMENT) | (j < SEGMENT)
    total = stats[0]
    for k in range(1, stats.shape[0]):
        total = total + stats[k]
    center_row = total[0:1] / full
    spread_row = total[1:2] / full - center_row * center_row
    scale_row = lax.rsqrt(spread_row + EPS)
    biases = [jnp.broadcast_to(bias[g : g + 1, :].astype(F32), (BLOCK, BLOCK)).T for g in range(width // GROUP_DIM)]
    for block in range(act_v.shape[0] // BLOCK):
        rows = pl.ds(block * BLOCK, BLOCK)
        at = slice(block * BLOCK, (block + 1) * BLOCK)
        center = jnp.broadcast_to(center_row[:, at], (BLOCK, BLOCK)).T
        scale = jnp.broadcast_to(scale_row[:, at], (BLOCK, BLOCK)).T
        for g in range(width // GROUP_DIM):
            cols = slice(g * GROUP_DIM, (g + 1) * GROUP_DIM)
            mixed = ((act_v[rows, cols] - center) * scale * gain[:, cols].astype(F32) + shift[:, cols].astype(F32)).astype(BF16)
            seen = jnp.where(visible, mix[g].astype(F32), 0.0).astype(BF16)
            spatial = jnp.dot(seen, mixed, preferred_element_type=F32) + biases[g]
            gated[rows, cols] = (act_u[rows, cols] * spatial).astype(BF16)
    c = place[1]
    for out, side in ((give, 1 - c), (keep, c)):
        for x in range(out.shape[0]):
            start = pl.multiple_of((2 * x + side) * width, width)
            columns = weight[pl.ds(start, width), :]
            out[x] = lax.dot_general(
                gated[...], columns, (((1,), (1,)), ((), ())), preferred_element_type=F32
            ).astype(BF16)


def shifted(value, by):
    row = lax.broadcasted_iota(jnp.int32, value.shape, 0)
    return jnp.where(row >= by, pltpu.roll(value, by, 0), 0.0)


def taps(value, weights):
    value = value.astype(BF16).astype(F32)
    return (shifted(value, 2) * weights[0:1] + shifted(value, 1) * weights[1:2]) + value * weights[2:3]


def ffn_kernel(place, mine, other, gain, late_hbm, conv_gate, conv_value, give, keep, normed, hidden, late, done):
    width = mine.shape[2]
    ff = conv_gate.shape[1]
    c = place[1]
    copies = [
        pltpu.make_async_copy(late_hbm.at[:, pl.ds(k * ff, ff)], late.at[:, pl.ds(k * ff, ff)], done.at[k])
        for k in range(3)
    ]
    for copy in copies:
        copy.start()
    for part in range(mine.shape[1] // SEQ_LEN):
        rows = pl.ds(part * SEQ_LEN, SEQ_LEN)
        squares = jnp.zeros((SEQ_LEN, 1), F32)
        for x in range(mine.shape[0]):
            for ref in (mine, other):
                value = ref[x, rows, :].astype(F32)
                squares = squares + jnp.sum(value * value, axis=1, keepdims=True)
        scale = lax.rsqrt(squares / (2 * mine.shape[0] * width) + EPS)

        def fill(ref, side):
            for x in range(mine.shape[0]):
                at = pl.ds((2 * x + side) * width, width)
                row = gain[2 * x + side, 0:1, :].astype(F32)
                normed[:, at] = (ref[x, rows, :].astype(F32) * scale * row).astype(BF16)

        @pl.when(c == 0)
        def _():
            fill(mine, 0)
            fill(other, 1)

        @pl.when(c == 1)
        def _():
            fill(other, 0)
            fill(mine, 1)

        if part == 0:
            copies[0].wait()
        gate = jnp.dot(normed[...], late[:, 0:ff], preferred_element_type=F32)
        if part == 0:
            copies[1].wait()
        value = jnp.dot(normed[...], late[:, ff : 2 * ff], preferred_element_type=F32)
        conv_g = taps(gate, conv_gate[...].astype(F32))
        conv_v = taps(value, conv_value[...].astype(F32))
        hidden[rows, :] = (conv_g * jax.nn.sigmoid(conv_g) * conv_v).astype(BF16)
    copies[2].wait()
    for out, side in ((give, 1 - c), (keep, c)):
        for x in range(out.shape[0]):
            start = pl.multiple_of((2 * x + side) * width, width)
            columns = late[pl.ds(start, width), 2 * ff : 3 * ff]
            out[x] = lax.dot_general(
                hidden[...], columns, (((1,), (1,)), ((), ())), preferred_element_type=F32
            ).astype(BF16)


def gelu(value):
    return 0.5 * value * (1.0 + lax.erf(value * SQRT_HALF))


def shape(dims, dtype):
    return jax.ShapeDtypeStruct(dims, dtype)


def room(mebibytes):
    return pltpu.CompilerParams(vmem_limit_bytes=mebibytes << 20)


def summed_at_owner(give, keep):
    pair = (keep.astype(F32) + other_core(give).astype(F32)).astype(BF16)
    arrived = lax.all_to_all(pair, "x", split_axis=0, concat_axis=0, tiled=True)
    return arrived.astype(F32).sum(axis=0)


def on_device(
    tokens,
    norm_gain,
    proj_u,
    proj_v,
    layer_gain,
    layer_shift,
    mix_weight,
    mix_bias,
    proj_out,
    ffn_gain,
    ffn_gate,
    ffn_value,
    conv_gate,
    conv_value,
    proj_down,
):
    da = proj_u.shape[1]
    ff = ffn_gate.shape[1]
    row_count = tokens.shape[0]

    early = jnp.concatenate([proj_u, proj_v, proj_out.T], axis=1)
    early_far = everyones(early, "zh").reshape(-1, early.shape[1])
    early_z = jnp.stack(round_ring(early_far, Z))
    early_all = everyones(early_z, "y").reshape(4, -1, early.shape[1])

    late = jnp.concatenate([ffn_gate, ffn_value, proj_down.T], axis=1)
    late_y = in_order(round_ring(late, "y"), "y").reshape(-1, late.shape[1])
    late_all = lax.all_gather(after(late_y, early_z), Z, axis=0, tiled=True)

    packed = jnp.concatenate([tokens, jnp.broadcast_to(norm_gain, (8, da)), jnp.broadcast_to(ffn_gain, (8, da))], axis=0)
    mine = round_ring(packed, "x")
    other = [other_core(part) for part in mine]
    place = jnp.stack([lax.axis_index(name).astype(jnp.int32) for name in ("x", "c", "zl")])
    model = proj_u.shape[0] * lax.axis_size(FS)
    tp = lax.axis_size(TP)
    normed, gain_two = pl.pallas_call(
        norm_kernel,
        in_specs=[SMEM] + [VMEM] * 8,
        out_specs=[VMEM] * 2,
        out_shape=[shape((row_count, model), BF16), shape((tp, 8, da), BF16)],
        name="norm",
        compiler_params=room(12),
    )(place, *mine, *other)

    act_v, sums = pl.pallas_call(
        stats_kernel,
        in_specs=[SMEM] + [VMEM] * 2,
        out_specs=[VMEM] * 2,
        out_shape=[shape((row_count, da), F32), shape((2, row_count), F32)],
        scratch_shapes=[pltpu.VMEM((model, da), BF16)],
        name="stats",
        compiler_params=room(14),
    )(place, normed, early_all)
    stats = everyones(sums, TP)
    act_u = pl.pallas_call(
        gate_kernel,
        in_specs=[SMEM] + [VMEM] * 2,
        out_specs=VMEM,
        out_shape=shape((row_count, da), F32),
        scratch_shapes=[pltpu.VMEM((model, da), BF16)],
        name="gate",
        compiler_params=room(14),
    )(place, normed, early_all)
    blocks = [shape((lax.axis_size("x"), row_count, da), BF16)] * 2
    give, keep = pl.pallas_call(
        mix_kernel,
        in_specs=[SMEM] + [VMEM] * 8,
        out_specs=[VMEM] * 2,
        out_shape=blocks,
        scratch_shapes=[pltpu.VMEM((model, da), BF16), pltpu.VMEM((row_count, da), BF16)],
        name="mix",
        compiler_params=room(16),
    )(
        place,
        act_v,
        act_u,
        stats,
        layer_gain[None],
        layer_shift[None],
        mix_weight,
        mix_bias,
        early_all,
    )
    stream = (tokens.astype(F32) + summed_at_owner(give, keep)).astype(BF16)
    mine = everyones(stream, "x")
    give, keep = pl.pallas_call(
        ffn_kernel,
        in_specs=[SMEM] + [VMEM] * 3 + [HBM] + [VMEM] * 2,
        out_specs=[VMEM] * 2,
        out_shape=blocks,
        scratch_shapes=[pltpu.VMEM((SEQ_LEN, model), BF16), pltpu.VMEM((row_count, ff), BF16), pltpu.VMEM(late_all.shape, BF16), pltpu.SemaphoreType.DMA((3,))],
        name="ffn",
        compiler_params=room(47),
    )(
        place,
        mine,
        other_core(mine),
        gain_two,
        late_all,
        conv_gate,
        conv_value,
    )
    return (stream.astype(F32) + summed_at_owner(give, keep)).astype(BF16)


def solution(mesh):
    split = Mesh(mesh.devices.reshape(4, 4, 4, 4, 2), ("zh", "zl", "y", "x", "c"))
    placed = (
        P(FS, TP),
        P(TP),
        P(FS, TP),
        P(FS, TP),
        P(TP),
        P(TP),
        P(TP, None, None),
        P(TP, None),
        P(TP, FS),
        P(TP),
        P(FS, TP),
        P(FS, TP),
        P(None, TP),
        P(None, TP),
        P(TP, FS),
    )

    return jax.shard_map(on_device, mesh=split, in_specs=placed, out_specs=P(FS, TP), check_vma=False)
```

```python
import jax
import jax.numpy as jnp
from jax import lax
from jax.experimental import pallas as pl
from jax.experimental.pallas import tpu as pltpu
from jax.sharding import Mesh
from jax.sharding import PartitionSpec as P

GROUP_DIM = 128
BLOCK = 128
SEGMENT = 64
SEQ_LEN = 256
Z = ("zh", "zl")
FS = ("zh", "zl", "y")
TP = ("x", "c")
EPS = 1e-06
F32 = jnp.float32
BF16 = jnp.bfloat16
SWAP = [(0, 1), (1, 0)]
RING = (0, 1, 3, 2)
PIECE = 32
HBM = pl.BlockSpec(memory_space=pltpu.HBM)
SQRT_HALF = 0.7071067811865476
VMEM = pl.BlockSpec(memory_space=pltpu.VMEM)
SMEM = pl.BlockSpec(memory_space=pltpu.SMEM)


def everyones(shard, axis):
    copies = jnp.broadcast_to(shard, (lax.axis_size(axis), *shard.shape))
    return lax.all_to_all(copies, axis, split_axis=0, concat_axis=0, tiled=True)


def other_core(value):
    return lax.ppermute(value, "c", SWAP)


def after(value, *first):
    return lax.optimization_barrier((value, *first))[0]


def round_ring(shard, axis):
    size = lax.axis_size(axis)
    steps = (1, size - 1, 2)
    return [shard] + [lax.ppermute(shard, axis, [(i, (i + step) % size) for i in range(size)]) for step in steps]


def doubled(blocks, step):
    came = lax.ppermute(blocks, "y", [(i, i ^ step) for i in range(4)])
    upper = (lax.axis_index("y") & step) != 0
    return jnp.concatenate([jnp.where(upper, came, blocks), jnp.where(upper, blocks, came)], axis=0)


def norm_kernel(place, p0, p1, p2, p3, out, gain_two):
    parts = (p0, p1, p2, p3)
    count, width = p0.shape[1] - 16, p0.shape[2]
    x, c = place[0], place[1]
    for part in range(count // BLOCK):
        rows = pl.ds(part * BLOCK, BLOCK)
        squares = jnp.zeros((BLOCK, width), F32)
        for ref in parts:
            for side in range(2):
                value = ref[side, rows, :].astype(F32)
                squares = squares + value * value
        scale = lax.rsqrt(jnp.sum(squares, axis=1, keepdims=True) / (8 * width) + EPS)
        for step, ref in zip(RING, parts):
            for side in range(2):
                block = origin(x, step) * 2 + (1 - c if side else c)
                gain = ref[side, count : count + 1, :].astype(F32)
                out[rows, pl.ds(pl.multiple_of(block * width, width), width)] = (
                    ref[side, rows, :].astype(F32) * scale * gain
                ).astype(BF16)
    for step, ref in zip(RING, parts):
        for side in range(2):
            block = origin(x, step) * 2 + (1 - c if side else c)
            gain_two[block] = ref[side, count + 8 : count + 16, :]


def origin(here, step):
    return (here + (4 - step)) & 3


def fill_rows(weight, parts, y, z):
    for step, part in zip(RING, parts):
        for at, less in enumerate(RING):
            for far in range(4):
                start = pl.multiple_of(((far * 4 + origin(z, less)) * 4 + origin(y, step)) * PIECE, PIECE)
                came = (at * 4 + far) * PIECE
                weight[pl.ds(start, PIECE), :] = part[came : came + PIECE, :]


def first_kernel(place, normed, p0, p1, p2, p3, act_u, act_v, sums, weight):
    width = act_u.shape[1]
    fill_rows(weight, (p0, p1, p2, p3), place[2], place[3])
    for part in range(normed.shape[0] // SEQ_LEN):
        rows = pl.ds(part * SEQ_LEN, SEQ_LEN)
        both = gelu(jnp.dot(normed[rows, :], weight[...], preferred_element_type=F32))
        act_u[rows, :] = both[:, :width]
        value = both[:, width:]
        act_v[rows, :] = value
        once = sum(value[:, k : k + 128] for k in range(0, width, 128))
        twice = sum(value[:, k : k + 128] * value[:, k : k + 128] for k in range(0, width, 128))
        sums[0:1, rows] = jnp.sum(once.T, axis=0, keepdims=True)
        sums[1:2, rows] = jnp.sum(twice.T, axis=0, keepdims=True)


def mix_kernel(place, act_v, act_u, stats, gain, shift, mix, bias, p0, p1, p2, p3, give, keep, weight, gated):
    width = act_v.shape[1]
    fill_rows(weight, (p0, p1, p2, p3), place[2], place[3])
    full = width * stats.shape[0]
    i = lax.broadcasted_iota(jnp.int32, (BLOCK, BLOCK), 0)
    j = lax.broadcasted_iota(jnp.int32, (BLOCK, BLOCK), 1)
    visible = (i >= SEGMENT) | (j < SEGMENT)
    total = stats[0]
    for k in range(1, stats.shape[0]):
        total = total + stats[k]
    center_row = total[0:1] / full
    spread_row = total[1:2] / full - center_row * center_row
    scale_row = lax.rsqrt(spread_row + EPS)
    biases = [jnp.broadcast_to(bias[g : g + 1, :].astype(F32), (BLOCK, BLOCK)).T for g in range(width // GROUP_DIM)]
    for block in range(act_v.shape[0] // BLOCK):
        rows = pl.ds(block * BLOCK, BLOCK)
        at = slice(block * BLOCK, (block + 1) * BLOCK)
        center = jnp.broadcast_to(center_row[:, at], (BLOCK, BLOCK)).T
        scale = jnp.broadcast_to(scale_row[:, at], (BLOCK, BLOCK)).T
        for g in range(width // GROUP_DIM):
            cols = slice(g * GROUP_DIM, (g + 1) * GROUP_DIM)
            mixed = ((act_v[rows, cols] - center) * scale * gain[:, cols].astype(F32) + shift[:, cols].astype(F32)).astype(BF16)
            seen = jnp.where(visible, mix[g].astype(F32), 0.0).astype(BF16)
            spatial = jnp.dot(seen, mixed, preferred_element_type=F32) + biases[g]
            gated[rows, cols] = (act_u[rows, cols] * spatial).astype(BF16)
    c = place[1]
    for out, side in ((give, 1 - c), (keep, c)):
        for x in range(out.shape[0]):
            start = pl.multiple_of((2 * x + side) * width, width)
            columns = weight[pl.ds(start, width), :]
            out[x] = lax.dot_general(
                gated[...], columns, (((1,), (1,)), ((), ())), preferred_element_type=F32
            ).astype(BF16)


def shifted(value, by):
    row = lax.broadcasted_iota(jnp.int32, value.shape, 0)
    return jnp.where(row >= by, pltpu.roll(value, by, 0), 0.0)


def taps(value, weights):
    value = value.astype(BF16).astype(F32)
    return (shifted(value, 2) * weights[0:1] + shifted(value, 1) * weights[1:2]) + value * weights[2:3]


def ffn_kernel(place, mine, other, gain, late_hbm, conv_gate, conv_value, give, keep, normed, hidden, late, done):
    width = mine.shape[2]
    ff = conv_gate.shape[1]
    c = place[1]
    copies = [
        pltpu.make_async_copy(late_hbm.at[:, pl.ds(k * ff, ff)], late.at[:, pl.ds(k * ff, ff)], done.at[k])
        for k in range(3)
    ]
    for copy in copies:
        copy.start()
    for part in range(mine.shape[1] // SEQ_LEN):
        rows = pl.ds(part * SEQ_LEN, SEQ_LEN)
        squares = jnp.zeros((SEQ_LEN, 1), F32)
        for x in range(mine.shape[0]):
            for ref in (mine, other):
                value = ref[x, rows, :].astype(F32)
                squares = squares + jnp.sum(value * value, axis=1, keepdims=True)
        scale = lax.rsqrt(squares / (2 * mine.shape[0] * width) + EPS)

        def fill(ref, side):
            for x in range(mine.shape[0]):
                at = pl.ds((2 * x + side) * width, width)
                row = gain[2 * x + side, 0:1, :].astype(F32)
                normed[:, at] = (ref[x, rows, :].astype(F32) * scale * row).astype(BF16)

        @pl.when(c == 0)
        def _():
            fill(mine, 0)
            fill(other, 1)

        @pl.when(c == 1)
        def _():
            fill(other, 0)
            fill(mine, 1)

        if part == 0:
            copies[0].wait()
        gate = jnp.dot(normed[...], late[:, 0:ff], preferred_element_type=F32)
        if part == 0:
            copies[1].wait()
        value = jnp.dot(normed[...], late[:, ff : 2 * ff], preferred_element_type=F32)
        conv_g = taps(gate, conv_gate[...].astype(F32))
        conv_v = taps(value, conv_value[...].astype(F32))
        hidden[rows, :] = (conv_g * jax.nn.sigmoid(conv_g) * conv_v).astype(BF16)
    copies[2].wait()
    for out, side in ((give, 1 - c), (keep, c)):
        for x in range(out.shape[0]):
            start = pl.multiple_of((2 * x + side) * width, width)
            columns = late[pl.ds(start, width), 2 * ff : 3 * ff]
            out[x] = lax.dot_general(
                hidden[...], columns, (((1,), (1,)), ((), ())), preferred_element_type=F32
            ).astype(BF16)


def gelu(value):
    return 0.5 * value * (1.0 + lax.erf(value * SQRT_HALF))


def shape(dims, dtype):
    return jax.ShapeDtypeStruct(dims, dtype)


def room(mebibytes):
    return pltpu.CompilerParams(vmem_limit_bytes=mebibytes << 20)


def summed_at_owner(give, keep):
    pair = (keep.astype(F32) + other_core(give).astype(F32)).astype(BF16)
    arrived = lax.all_to_all(pair, "x", split_axis=0, concat_axis=0, tiled=True)
    return arrived.astype(F32).sum(axis=0)


def on_device(
    tokens,
    norm_gain,
    proj_u,
    proj_v,
    layer_gain,
    layer_shift,
    mix_weight,
    mix_bias,
    proj_out,
    ffn_gain,
    ffn_gate,
    ffn_value,
    conv_gate,
    conv_value,
    proj_down,
):
    da = proj_u.shape[1]
    ff = ffn_gate.shape[1]
    row_count = tokens.shape[0]

    early = jnp.concatenate([proj_u, proj_v, proj_out.T], axis=1)
    early_far = everyones(early, "zh").reshape(-1, early.shape[1])
    early_z = round_ring(early_far, Z)
    early_parts = round_ring(jnp.concatenate([part[:, : 2 * da] for part in early_z], axis=0), "y")
    out_parts = round_ring(jnp.concatenate([part[:, 2 * da :] for part in early_z], axis=0), "y")

    late = jnp.concatenate([ffn_gate, ffn_value, proj_down.T], axis=1)
    late_pair = doubled(late[None], 1)
    late_y = doubled(late_pair, 2).reshape(-1, late.shape[1])
    late_all = lax.all_gather(after(late_y, *early_z), Z, axis=0, tiled=True)

    packed = jnp.concatenate([tokens, jnp.broadcast_to(norm_gain, (8, da)), jnp.broadcast_to(ffn_gain, (8, da))], axis=0)
    pair = jnp.stack([packed, other_core(packed)])
    token_parts = round_ring(pair, "x")
    place = jnp.stack([lax.axis_index(name).astype(jnp.int32) for name in ("x", "c", "y", "zl")])
    model = proj_u.shape[0] * lax.axis_size(FS)
    tp = lax.axis_size(TP)
    normed, gain_two = pl.pallas_call(
        norm_kernel,
        in_specs=[SMEM] + [VMEM] * 4,
        out_specs=[VMEM] * 2,
        out_shape=[shape((row_count, model), BF16), shape((tp, 8, da), BF16)],
        name="norm",
        compiler_params=room(12),
    )(place, *token_parts)

    act_u, act_v, sums = pl.pallas_call(
        first_kernel,
        in_specs=[SMEM] + [VMEM] * 5,
        out_specs=[VMEM] * 3,
        out_shape=[shape((row_count, da), F32)] * 2 + [shape((2, row_count), F32)],
        scratch_shapes=[pltpu.VMEM((model, 2 * da), BF16)],
        name="first",
        compiler_params=room(14),
    )(place, normed, *early_parts)
    stats = everyones(sums, TP)
    blocks = [shape((lax.axis_size("x"), row_count, da), BF16)] * 2
    give, keep = pl.pallas_call(
        mix_kernel,
        in_specs=[SMEM] + [VMEM] * 11,
        out_specs=[VMEM] * 2,
        out_shape=blocks,
        scratch_shapes=[pltpu.VMEM((model, da), BF16), pltpu.VMEM((row_count, da), BF16)],
        name="mix",
        compiler_params=room(16),
    )(
        place,
        act_v,
        act_u,
        stats,
        layer_gain[None],
        layer_shift[None],
        mix_weight,
        mix_bias,
        *out_parts,
    )
    stream = (tokens.astype(F32) + summed_at_owner(give, keep)).astype(BF16)
    mine = everyones(stream, "x")
    give, keep = pl.pallas_call(
        ffn_kernel,
        in_specs=[SMEM] + [VMEM] * 3 + [HBM] + [VMEM] * 2,
        out_specs=[VMEM] * 2,
        out_shape=blocks,
        scratch_shapes=[pltpu.VMEM((SEQ_LEN, model), BF16), pltpu.VMEM((row_count, ff), BF16), pltpu.VMEM(late_all.shape, BF16), pltpu.SemaphoreType.DMA((3,))],
        name="ffn",
        compiler_params=room(47),
    )(
        place,
        mine,
        other_core(mine),
        gain_two,
        late_all,
        conv_gate,
        conv_value,
    )
    return (stream.astype(F32) + summed_at_owner(give, keep)).astype(BF16)


def solution(mesh):
    split = Mesh(mesh.devices.reshape(4, 4, 4, 4, 2), ("zh", "zl", "y", "x", "c"))
    placed = (
        P(FS, TP),
        P(TP),
        P(FS, TP),
        P(FS, TP),
        P(TP),
        P(TP),
        P(TP, None, None),
        P(TP, None),
        P(TP, FS),
        P(TP),
        P(FS, TP),
        P(FS, TP),
        P(None, TP),
        P(None, TP),
        P(TP, FS),
    )

    return jax.shard_map(on_device, mesh=split, in_specs=placed, out_specs=P(FS, TP), check_vma=False)
```

```python
import jax
import jax.numpy as jnp
from jax import lax
from jax.experimental import pallas as pl
from jax.experimental.pallas import tpu as pltpu
from jax.sharding import Mesh
from jax.sharding import PartitionSpec as P

GROUP_DIM = 128
BLOCK = 128
SEGMENT = 64
SEQ_LEN = 256
Z = ("zh", "zl")
FS = ("zh", "zl", "y")
TP = ("x", "c")
EPS = 1e-06
F32 = jnp.float32
BF16 = jnp.bfloat16
SWAP = [(0, 1), (1, 0)]
RING = (0, 1, 3, 2)
PIECE = 32
HBM = pl.BlockSpec(memory_space=pltpu.HBM)
SQRT_HALF = 0.7071067811865476
VMEM = pl.BlockSpec(memory_space=pltpu.VMEM)
SMEM = pl.BlockSpec(memory_space=pltpu.SMEM)


def everyones(shard, axis):
    copies = jnp.broadcast_to(shard, (lax.axis_size(axis), *shard.shape))
    return lax.all_to_all(copies, axis, split_axis=0, concat_axis=0, tiled=True)


def other_core(value):
    return lax.ppermute(value, "c", SWAP)


def after(value, *first):
    return lax.optimization_barrier((value, *first))[0]


def round_ring(shard, axis):
    size = lax.axis_size(axis)
    steps = (1, size - 1, 2)
    return [shard] + [lax.ppermute(shard, axis, [(i, (i + step) % size) for i in range(size)]) for step in steps]


def norm_kernel(place, mine, other, out, gain_two):
    count, width = mine.shape[1] - 16, mine.shape[2]
    c = place[0]
    blocks = [(ref, x, 2 * x + (1 - c if side else c)) for side, ref in enumerate((mine, other)) for x in range(4)]
    for part in range(count // BLOCK):
        rows = pl.ds(part * BLOCK, BLOCK)
        squares = jnp.zeros((BLOCK, width), F32)
        for ref, x, _ in blocks:
            value = ref[x, rows, :].astype(F32)
            squares = squares + value * value
        scale = lax.rsqrt(jnp.sum(squares, axis=1, keepdims=True) / (8 * width) + EPS)
        for ref, x, block in blocks:
            gain = ref[x, count : count + 1, :].astype(F32)
            out[rows, pl.ds(pl.multiple_of(block * width, width), width)] = (
                ref[x, rows, :].astype(F32) * scale * gain
            ).astype(BF16)
    for ref, x, block in blocks:
        gain_two[block] = ref[x, count + 8 : count + 16, :]


def origin(here, step):
    return (here + (4 - step)) & 3


def fill_rows(weight, parts, y, z):
    for step, part in zip(RING, parts):
        for at, less in enumerate(RING):
            for far in range(4):
                start = pl.multiple_of(((far * 4 + origin(z, less)) * 4 + origin(y, step)) * PIECE, PIECE)
                came = (at * 4 + far) * PIECE
                weight[pl.ds(start, PIECE), :] = part[came : came + PIECE, :]


def first_kernel(place, normed, p0, p1, p2, p3, act_u, act_v, sums, weight):
    width = act_u.shape[1]
    fill_rows(weight, (p0, p1, p2, p3), place[1], place[2])
    for part in range(normed.shape[0] // SEQ_LEN):
        rows = pl.ds(part * SEQ_LEN, SEQ_LEN)
        both = gelu(jnp.dot(normed[rows, :], weight[...], preferred_element_type=F32))
        act_u[rows, :] = both[:, :width]
        value = both[:, width:]
        act_v[rows, :] = value
        once = sum(value[:, k : k + 128] for k in range(0, width, 128))
        twice = sum(value[:, k : k + 128] * value[:, k : k + 128] for k in range(0, width, 128))
        sums[0:1, rows] = jnp.sum(once.T, axis=0, keepdims=True)
        sums[1:2, rows] = jnp.sum(twice.T, axis=0, keepdims=True)


def mix_kernel(place, act_v, act_u, stats, gain, shift, mix, bias, p0, p1, p2, p3, give, keep, weight, gated):
    width = act_v.shape[1]
    fill_rows(weight, (p0, p1, p2, p3), place[1], place[2])
    full = width * stats.shape[0]
    i = lax.broadcasted_iota(jnp.int32, (BLOCK, BLOCK), 0)
    j = lax.broadcasted_iota(jnp.int32, (BLOCK, BLOCK), 1)
    visible = (i >= SEGMENT) | (j < SEGMENT)
    total = stats[0]
    for k in range(1, stats.shape[0]):
        total = total + stats[k]
    center_row = total[0:1] / full
    spread_row = total[1:2] / full - center_row * center_row
    scale_row = lax.rsqrt(spread_row + EPS)
    biases = [jnp.broadcast_to(bias[g : g + 1, :].astype(F32), (BLOCK, BLOCK)).T for g in range(width // GROUP_DIM)]
    for block in range(act_v.shape[0] // BLOCK):
        rows = pl.ds(block * BLOCK, BLOCK)
        at = slice(block * BLOCK, (block + 1) * BLOCK)
        center = jnp.broadcast_to(center_row[:, at], (BLOCK, BLOCK)).T
        scale = jnp.broadcast_to(scale_row[:, at], (BLOCK, BLOCK)).T
        for g in range(width // GROUP_DIM):
            cols = slice(g * GROUP_DIM, (g + 1) * GROUP_DIM)
            mixed = ((act_v[rows, cols] - center) * scale * gain[:, cols].astype(F32) + shift[:, cols].astype(F32)).astype(BF16)
            seen = jnp.where(visible, mix[g].astype(F32), 0.0).astype(BF16)
            spatial = jnp.dot(seen, mixed, preferred_element_type=F32) + biases[g]
            gated[rows, cols] = (act_u[rows, cols] * spatial).astype(BF16)
    c = place[0]
    for out, side in ((give, 1 - c), (keep, c)):
        for x in range(out.shape[0]):
            start = pl.multiple_of((2 * x + side) * width, width)
            columns = weight[pl.ds(start, width), :]
            out[x] = lax.dot_general(
                gated[...], columns, (((1,), (1,)), ((), ())), preferred_element_type=F32
            ).astype(BF16)


def shifted(value, by):
    row = lax.broadcasted_iota(jnp.int32, value.shape, 0)
    return jnp.where(row >= by, pltpu.roll(value, by, 0), 0.0)


def taps(value, weights):
    value = value.astype(BF16).astype(F32)
    return (shifted(value, 2) * weights[0:1] + shifted(value, 1) * weights[1:2]) + value * weights[2:3]


def ffn_kernel(place, mine, other, gain, late_hbm, conv_gate, conv_value, give, keep, normed, hidden, late, done):
    width = mine.shape[2]
    ff = conv_gate.shape[1]
    c = place[0]
    copies = [
        pltpu.make_async_copy(late_hbm.at[:, pl.ds(k * ff, ff)], late.at[:, pl.ds(k * ff, ff)], done.at[k])
        for k in range(3)
    ]
    for copy in copies:
        copy.start()
    for part in range(mine.shape[1] // SEQ_LEN):
        rows = pl.ds(part * SEQ_LEN, SEQ_LEN)
        squares = jnp.zeros((SEQ_LEN, 1), F32)
        for x in range(mine.shape[0]):
            for ref in (mine, other):
                value = ref[x, rows, :].astype(F32)
                squares = squares + jnp.sum(value * value, axis=1, keepdims=True)
        scale = lax.rsqrt(squares / (2 * mine.shape[0] * width) + EPS)

        def fill(ref, side):
            for x in range(mine.shape[0]):
                at = pl.ds((2 * x + side) * width, width)
                row = gain[2 * x + side, 0:1, :].astype(F32)
                normed[:, at] = (ref[x, rows, :].astype(F32) * scale * row).astype(BF16)

        @pl.when(c == 0)
        def _():
            fill(mine, 0)
            fill(other, 1)

        @pl.when(c == 1)
        def _():
            fill(other, 0)
            fill(mine, 1)

        if part == 0:
            copies[0].wait()
        gate = jnp.dot(normed[...], late[:, 0:ff], preferred_element_type=F32)
        if part == 0:
            copies[1].wait()
        value = jnp.dot(normed[...], late[:, ff : 2 * ff], preferred_element_type=F32)
        conv_g = taps(gate, conv_gate[...].astype(F32))
        conv_v = taps(value, conv_value[...].astype(F32))
        hidden[rows, :] = (conv_g * jax.nn.sigmoid(conv_g) * conv_v).astype(BF16)
    copies[2].wait()
    for out, side in ((give, 1 - c), (keep, c)):
        for x in range(out.shape[0]):
            start = pl.multiple_of((2 * x + side) * width, width)
            columns = late[pl.ds(start, width), 2 * ff : 3 * ff]
            out[x] = lax.dot_general(
                hidden[...], columns, (((1,), (1,)), ((), ())), preferred_element_type=F32
            ).astype(BF16)


def gelu(value):
    return 0.5 * value * (1.0 + lax.erf(value * SQRT_HALF))


def shape(dims, dtype):
    return jax.ShapeDtypeStruct(dims, dtype)


def room(mebibytes):
    return pltpu.CompilerParams(vmem_limit_bytes=mebibytes << 20)


def summed_at_owner(give, keep):
    pair = (keep.astype(F32) + other_core(give).astype(F32)).astype(BF16)
    arrived = lax.all_to_all(pair, "x", split_axis=0, concat_axis=0, tiled=True)
    return arrived.astype(F32).sum(axis=0)


def on_device(
    tokens,
    norm_gain,
    proj_u,
    proj_v,
    layer_gain,
    layer_shift,
    mix_weight,
    mix_bias,
    proj_out,
    ffn_gain,
    ffn_gate,
    ffn_value,
    conv_gate,
    conv_value,
    proj_down,
):
    da = proj_u.shape[1]
    ff = ffn_gate.shape[1]
    row_count = tokens.shape[0]

    early = jnp.concatenate([proj_u, proj_v, proj_out.T], axis=1)
    early_far = everyones(early, "zh").reshape(-1, early.shape[1])
    early_z = jnp.concatenate(round_ring(early_far, Z), axis=0)
    early_parts = round_ring(early_z[:, : 2 * da], "y")
    out_parts = round_ring(early_z[:, 2 * da :], "y")

    late = jnp.concatenate([ffn_gate, ffn_value, proj_down.T], axis=1)
    padded = jnp.pad(late, ((0, 2 * late.shape[0]), (0, 0)))
    late_y = lax.all_gather(padded, "y", axis=0)[:, : late.shape[0]].reshape(-1, late.shape[1])
    late_all = lax.all_gather(after(late_y, early_z), Z, axis=0, tiled=True)

    packed = jnp.concatenate([tokens, jnp.broadcast_to(norm_gain, (8, da)), jnp.broadcast_to(ffn_gain, (8, da))], axis=0)
    mine = lax.all_gather(packed, "x", axis=0)
    other = other_core(mine)
    place = jnp.stack([lax.axis_index(name).astype(jnp.int32) for name in ("c", "y", "zl")])
    model = proj_u.shape[0] * lax.axis_size(FS)
    tp = lax.axis_size(TP)
    normed, gain_two = pl.pallas_call(
        norm_kernel,
        in_specs=[SMEM] + [VMEM] * 2,
        out_specs=[VMEM] * 2,
        out_shape=[shape((row_count, model), BF16), shape((tp, 8, da), BF16)],
        name="norm",
        compiler_params=room(12),
    )(place, mine, other)

    act_u, act_v, sums = pl.pallas_call(
        first_kernel,
        in_specs=[SMEM] + [VMEM] * 5,
        out_specs=[VMEM] * 3,
        out_shape=[shape((row_count, da), F32)] * 2 + [shape((2, row_count), F32)],
        scratch_shapes=[pltpu.VMEM((model, 2 * da), BF16)],
        name="first",
        compiler_params=room(14),
    )(place, normed, *early_parts)
    stats = everyones(sums, TP)
    blocks = [shape((lax.axis_size("x"), row_count, da), BF16)] * 2
    give, keep = pl.pallas_call(
        mix_kernel,
        in_specs=[SMEM] + [VMEM] * 11,
        out_specs=[VMEM] * 2,
        out_shape=blocks,
        scratch_shapes=[pltpu.VMEM((model, da), BF16), pltpu.VMEM((row_count, da), BF16)],
        name="mix",
        compiler_params=room(16),
    )(
        place,
        act_v,
        act_u,
        stats,
        layer_gain[None],
        layer_shift[None],
        mix_weight,
        mix_bias,
        *out_parts,
    )
    stream = (tokens.astype(F32) + summed_at_owner(give, keep)).astype(BF16)
    mine = everyones(stream, "x")
    give, keep = pl.pallas_call(
        ffn_kernel,
        in_specs=[SMEM] + [VMEM] * 3 + [HBM] + [VMEM] * 2,
        out_specs=[VMEM] * 2,
        out_shape=blocks,
        scratch_shapes=[pltpu.VMEM((SEQ_LEN, model), BF16), pltpu.VMEM((row_count, ff), BF16), pltpu.VMEM(late_all.shape, BF16), pltpu.SemaphoreType.DMA((3,))],
        name="ffn",
        compiler_params=room(47),
    )(
        place,
        mine,
        other_core(mine),
        gain_two,
        late_all,
        conv_gate,
        conv_value,
    )
    return (stream.astype(F32) + summed_at_owner(give, keep)).astype(BF16)


def solution(mesh):
    split = Mesh(mesh.devices.reshape(4, 4, 4, 4, 2), ("zh", "zl", "y", "x", "c"))
    placed = (
        P(FS, TP),
        P(TP),
        P(FS, TP),
        P(FS, TP),
        P(TP),
        P(TP),
        P(TP, None, None),
        P(TP, None),
        P(TP, FS),
        P(TP),
        P(FS, TP),
        P(FS, TP),
        P(None, TP),
        P(None, TP),
        P(TP, FS),
    )

    return jax.shard_map(on_device, mesh=split, in_specs=placed, out_specs=P(FS, TP), check_vma=False)
```

```python
import jax
import jax.numpy as jnp
from jax import lax
from jax.experimental import pallas as pl
from jax.experimental.pallas import tpu as pltpu
from jax.sharding import Mesh
from jax.sharding import PartitionSpec as P

GROUP_DIM = 128
BLOCK = 128
SEGMENT = 64
SEQ_LEN = 256
Z = ("zh", "zl")
FS = ("zh", "zl", "y")
TP = ("x", "c")
EPS = 1e-06
F32 = jnp.float32
BF16 = jnp.bfloat16
SWAP = [(0, 1), (1, 0)]
RING = (0, 1, 3, 2)
PIECE = 32
HBM = pl.BlockSpec(memory_space=pltpu.HBM)
SQRT_HALF = 0.7071067811865476
VMEM = pl.BlockSpec(memory_space=pltpu.VMEM)
SMEM = pl.BlockSpec(memory_space=pltpu.SMEM)


def everyones(shard, axis):
    copies = jnp.broadcast_to(shard, (lax.axis_size(axis), *shard.shape))
    return lax.all_to_all(copies, axis, split_axis=0, concat_axis=0, tiled=True)


def other_core(value):
    return lax.ppermute(value, "c", SWAP)


def after(value, *first):
    return lax.optimization_barrier((value, *first))[0]


def round_ring(shard, axis):
    size = lax.axis_size(axis)
    steps = (1, size - 1, 2)
    return [shard] + [lax.ppermute(shard, axis, [(i, (i + step) % size) for i in range(size)]) for step in steps]


def norm_kernel(place, p0, p1, p2, p3, out, gain_two):
    parts = (p0, p1, p2, p3)
    count, width = p0.shape[1] - 16, p0.shape[2]
    x, c = place[0], place[1]
    for part in range(count // BLOCK):
        rows = pl.ds(part * BLOCK, BLOCK)
        squares = jnp.zeros((BLOCK, width), F32)
        for ref in parts:
            for side in range(2):
                value = ref[side, rows, :].astype(F32)
                squares = squares + value * value
        scale = lax.rsqrt(jnp.sum(squares, axis=1, keepdims=True) / (8 * width) + EPS)
        for step, ref in zip(RING, parts):
            for side in range(2):
                block = origin(x, step) * 2 + (1 - c if side else c)
                gain = ref[side, count : count + 1, :].astype(F32)
                out[rows, pl.ds(pl.multiple_of(block * width, width), width)] = (
                    ref[side, rows, :].astype(F32) * scale * gain
                ).astype(BF16)
    for step, ref in zip(RING, parts):
        for side in range(2):
            block = origin(x, step) * 2 + (1 - c if side else c)
            gain_two[block] = ref[side, count + 8 : count + 16, :]


def origin(here, step):
    return (here + (4 - step)) & 3


def fill_rows(weight, parts, y, z):
    for step, part in zip(RING, parts):
        for at, less in enumerate(RING):
            for far in range(4):
                start = pl.multiple_of(((far * 4 + origin(z, less)) * 4 + origin(y, step)) * PIECE, PIECE)
                came = (at * 4 + far) * PIECE
                weight[pl.ds(start, PIECE), :] = part[came : came + PIECE, :]


def first_kernel(place, normed, p0, p1, p2, p3, act_u, act_v, sums, weight):
    width = act_u.shape[1]
    fill_rows(weight, (p0, p1, p2, p3), place[2], place[3])
    for part in range(normed.shape[0] // SEQ_LEN):
        rows = pl.ds(part * SEQ_LEN, SEQ_LEN)
        both = gelu(jnp.dot(normed[rows, :], weight[...], preferred_element_type=F32))
        act_u[rows, :] = both[:, :width]
        value = both[:, width:]
        act_v[rows, :] = value
        once = sum(value[:, k : k + 128] for k in range(0, width, 128))
        twice = sum(value[:, k : k + 128] * value[:, k : k + 128] for k in range(0, width, 128))
        sums[0:1, rows] = jnp.sum(once.T, axis=0, keepdims=True)
        sums[1:2, rows] = jnp.sum(twice.T, axis=0, keepdims=True)


def mix_kernel(place, act_v, act_u, stats, gain, shift, mix, bias, p0, p1, p2, p3, give, keep, weight, gated):
    width = act_v.shape[1]
    fill_rows(weight, (p0, p1, p2, p3), place[2], place[3])
    full = width * stats.shape[0]
    i = lax.broadcasted_iota(jnp.int32, (BLOCK, BLOCK), 0)
    j = lax.broadcasted_iota(jnp.int32, (BLOCK, BLOCK), 1)
    visible = (i >= SEGMENT) | (j < SEGMENT)
    total = stats[0]
    for k in range(1, stats.shape[0]):
        total = total + stats[k]
    center_row = total[0:1] / full
    spread_row = total[1:2] / full - center_row * center_row
    scale_row = lax.rsqrt(spread_row + EPS)
    biases = [jnp.broadcast_to(bias[g : g + 1, :].astype(F32), (BLOCK, BLOCK)).T for g in range(width // GROUP_DIM)]
    for block in range(act_v.shape[0] // BLOCK):
        rows = pl.ds(block * BLOCK, BLOCK)
        at = slice(block * BLOCK, (block + 1) * BLOCK)
        center = jnp.broadcast_to(center_row[:, at], (BLOCK, BLOCK)).T
        scale = jnp.broadcast_to(scale_row[:, at], (BLOCK, BLOCK)).T
        for g in range(width // GROUP_DIM):
            cols = slice(g * GROUP_DIM, (g + 1) * GROUP_DIM)
            mixed = ((act_v[rows, cols] - center) * scale * gain[:, cols].astype(F32) + shift[:, cols].astype(F32)).astype(BF16)
            seen = jnp.where(visible, mix[g].astype(F32), 0.0).astype(BF16)
            spatial = jnp.dot(seen, mixed, preferred_element_type=F32) + biases[g]
            gated[rows, cols] = (act_u[rows, cols] * spatial).astype(BF16)
    c = place[1]
    for out, side in ((give, 1 - c), (keep, c)):
        for x in range(out.shape[0]):
            start = pl.multiple_of((2 * x + side) * width, width)
            columns = weight[pl.ds(start, width), :]
            out[x] = lax.dot_general(
                gated[...], columns, (((1,), (1,)), ((), ())), preferred_element_type=F32
            ).astype(BF16)


def shifted(value, by):
    row = lax.broadcasted_iota(jnp.int32, value.shape, 0)
    return jnp.where(row >= by, pltpu.roll(value, by, 0), 0.0)


def taps(value, weights):
    value = value.astype(BF16).astype(F32)
    return (shifted(value, 2) * weights[0:1] + shifted(value, 1) * weights[1:2]) + value * weights[2:3]


def ffn_kernel(place, mine, other, gain, late_hbm, conv_gate, conv_value, give, keep, normed, hidden, late, done):
    width = mine.shape[2]
    ff = conv_gate.shape[1]
    c = place[1]
    copies = [
        pltpu.make_async_copy(late_hbm.at[:, pl.ds(k * ff, ff)], late.at[:, pl.ds(k * ff, ff)], done.at[k])
        for k in range(3)
    ]
    for copy in copies:
        copy.start()
    for part in range(mine.shape[1] // SEQ_LEN):
        rows = pl.ds(part * SEQ_LEN, SEQ_LEN)
        squares = jnp.zeros((SEQ_LEN, 1), F32)
        for x in range(mine.shape[0]):
            for ref in (mine, other):
                value = ref[x, rows, :].astype(F32)
                squares = squares + jnp.sum(value * value, axis=1, keepdims=True)
        scale = lax.rsqrt(squares / (2 * mine.shape[0] * width) + EPS)

        def fill(ref, side):
            for x in range(mine.shape[0]):
                at = pl.ds((2 * x + side) * width, width)
                row = gain[2 * x + side, 0:1, :].astype(F32)
                normed[:, at] = (ref[x, rows, :].astype(F32) * scale * row).astype(BF16)

        @pl.when(c == 0)
        def _():
            fill(mine, 0)
            fill(other, 1)

        @pl.when(c == 1)
        def _():
            fill(other, 0)
            fill(mine, 1)

        if part == 0:
            copies[0].wait()
        gate = jnp.dot(normed[...], late[:, 0:ff], preferred_element_type=F32)
        if part == 0:
            copies[1].wait()
        value = jnp.dot(normed[...], late[:, ff : 2 * ff], preferred_element_type=F32)
        conv_g = taps(gate, conv_gate[...].astype(F32))
        conv_v = taps(value, conv_value[...].astype(F32))
        hidden[rows, :] = (conv_g * jax.nn.sigmoid(conv_g) * conv_v).astype(BF16)
    copies[2].wait()
    for out, side in ((give, 1 - c), (keep, c)):
        for x in range(out.shape[0]):
            start = pl.multiple_of((2 * x + side) * width, width)
            columns = late[pl.ds(start, width), 2 * ff : 3 * ff]
            out[x] = lax.dot_general(
                hidden[...], columns, (((1,), (1,)), ((), ())), preferred_element_type=F32
            ).astype(BF16)


def gelu(value):
    return 0.5 * value * (1.0 + lax.erf(value * SQRT_HALF))


def shape(dims, dtype):
    return jax.ShapeDtypeStruct(dims, dtype)


def room(mebibytes):
    return pltpu.CompilerParams(vmem_limit_bytes=mebibytes << 20)


def summed_at_owner(give, keep):
    pair = (keep.astype(F32) + other_core(give).astype(F32)).astype(BF16)
    arrived = lax.all_to_all(pair, "x", split_axis=0, concat_axis=0, tiled=True)
    return arrived.astype(F32).sum(axis=0)


def on_device(
    tokens,
    norm_gain,
    proj_u,
    proj_v,
    layer_gain,
    layer_shift,
    mix_weight,
    mix_bias,
    proj_out,
    ffn_gain,
    ffn_gate,
    ffn_value,
    conv_gate,
    conv_value,
    proj_down,
):
    da = proj_u.shape[1]
    ff = ffn_gate.shape[1]
    row_count = tokens.shape[0]

    early = jnp.concatenate([proj_u, proj_v, proj_out.T], axis=1)
    early_far = everyones(early, "zh").reshape(-1, early.shape[1])
    early_z = jnp.concatenate(round_ring(early_far, Z), axis=0)
    early_parts = round_ring(early_z[:, : 2 * da], "y")
    out_parts = round_ring(early_z[:, 2 * da :], "y")

    late = jnp.concatenate([ffn_gate, ffn_value, proj_down.T], axis=1)
    padded = jnp.pad(late, ((0, 2 * late.shape[0]), (0, 0)))
    late_y = lax.all_gather(padded, "y", axis=0)[:, : late.shape[0]].reshape(-1, late.shape[1])
    late_all = lax.all_gather(after(late_y, early_z), Z, axis=0, tiled=True)

    packed = jnp.concatenate([tokens, jnp.broadcast_to(norm_gain, (8, da)), jnp.broadcast_to(ffn_gain, (8, da))], axis=0)
    pair = jnp.stack([packed, other_core(packed)])
    token_parts = round_ring(pair, "x")
    place = jnp.stack([lax.axis_index(name).astype(jnp.int32) for name in ("x", "c", "y", "zl")])
    model = proj_u.shape[0] * lax.axis_size(FS)
    tp = lax.axis_size(TP)
    normed, gain_two = pl.pallas_call(
        norm_kernel,
        in_specs=[SMEM] + [VMEM] * 4,
        out_specs=[VMEM] * 2,
        out_shape=[shape((row_count, model), BF16), shape((tp, 8, da), BF16)],
        name="norm",
        compiler_params=room(12),
    )(place, *token_parts)

    act_u, act_v, sums = pl.pallas_call(
        first_kernel,
        in_specs=[SMEM] + [VMEM] * 5,
        out_specs=[VMEM] * 3,
        out_shape=[shape((row_count, da), F32)] * 2 + [shape((2, row_count), F32)],
        scratch_shapes=[pltpu.VMEM((model, 2 * da), BF16)],
        name="first",
        compiler_params=room(14),
    )(place, normed, *early_parts)
    stats = everyones(sums, TP)
    blocks = [shape((lax.axis_size("x"), row_count, da), BF16)] * 2
    give, keep = pl.pallas_call(
        mix_kernel,
        in_specs=[SMEM] + [VMEM] * 11,
        out_specs=[VMEM] * 2,
        out_shape=blocks,
        scratch_shapes=[pltpu.VMEM((model, da), BF16), pltpu.VMEM((row_count, da), BF16)],
        name="mix",
        compiler_params=room(16),
    )(
        place,
        act_v,
        act_u,
        stats,
        layer_gain[None],
        layer_shift[None],
        mix_weight,
        mix_bias,
        *out_parts,
    )
    stream = (tokens.astype(F32) + summed_at_owner(give, keep)).astype(BF16)
    mine = everyones(stream, "x")
    give, keep = pl.pallas_call(
        ffn_kernel,
        in_specs=[SMEM] + [VMEM] * 3 + [HBM] + [VMEM] * 2,
        out_specs=[VMEM] * 2,
        out_shape=blocks,
        scratch_shapes=[pltpu.VMEM((SEQ_LEN, model), BF16), pltpu.VMEM((row_count, ff), BF16), pltpu.VMEM(late_all.shape, BF16), pltpu.SemaphoreType.DMA((3,))],
        name="ffn",
        compiler_params=room(47),
    )(
        place,
        mine,
        other_core(mine),
        gain_two,
        late_all,
        conv_gate,
        conv_value,
    )
    return (stream.astype(F32) + summed_at_owner(give, keep)).astype(BF16)


def solution(mesh):
    split = Mesh(mesh.devices.reshape(4, 4, 4, 4, 2), ("zh", "zl", "y", "x", "c"))
    placed = (
        P(FS, TP),
        P(TP),
        P(FS, TP),
        P(FS, TP),
        P(TP),
        P(TP),
        P(TP, None, None),
        P(TP, None),
        P(TP, FS),
        P(TP),
        P(FS, TP),
        P(FS, TP),
        P(None, TP),
        P(None, TP),
        P(TP, FS),
    )

    return jax.shard_map(on_device, mesh=split, in_specs=placed, out_specs=P(FS, TP), check_vma=False)
```

```python
import jax
import jax.numpy as jnp
from jax import lax
from jax.experimental import pallas as pl
from jax.experimental.pallas import tpu as pltpu
from jax.sharding import Mesh
from jax.sharding import PartitionSpec as P

GROUP_DIM = 128
BLOCK = 128
SEGMENT = 64
SEQ_LEN = 256
Z = ("zh", "zl")
FS = ("zh", "zl", "y")
TP = ("x", "c")
EPS = 1e-06
F32 = jnp.float32
BF16 = jnp.bfloat16
SWAP = [(0, 1), (1, 0)]
RING = (0, 2, 1, 3)
PIECE = 32
HBM = pl.BlockSpec(memory_space=pltpu.HBM)
SQRT_HALF = 0.7071067811865476
VMEM = pl.BlockSpec(memory_space=pltpu.VMEM)
SMEM = pl.BlockSpec(memory_space=pltpu.SMEM)


def everyones(shard, axis):
    copies = jnp.broadcast_to(shard, (lax.axis_size(axis), *shard.shape))
    return lax.all_to_all(copies, axis, split_axis=0, concat_axis=0, tiled=True)


def other_core(value):
    return lax.ppermute(value, "c", SWAP)


def after(value, *first):
    return lax.optimization_barrier((value, *first))[0]


def round_ring(shard, axis):
    size = lax.axis_size(axis)
    steps = (2, 1, size - 1)
    return [shard] + [lax.ppermute(shard, axis, [(i, (i + step) % size) for i in range(size)]) for step in steps]


def norm_kernel(place, p0, p1, p2, p3, out, gain_two):
    parts = (p0, p1, p2, p3)
    count, width = p0.shape[1] - 16, p0.shape[2]
    x, c = place[0], place[1]
    for part in range(count // BLOCK):
        rows = pl.ds(part * BLOCK, BLOCK)
        squares = jnp.zeros((BLOCK, width), F32)
        for ref in parts:
            for side in range(2):
                value = ref[side, rows, :].astype(F32)
                squares = squares + value * value
        scale = lax.rsqrt(jnp.sum(squares, axis=1, keepdims=True) / (8 * width) + EPS)
        for step, ref in zip(RING, parts):
            for side in range(2):
                block = origin(x, step) * 2 + (1 - c if side else c)
                gain = ref[side, count : count + 1, :].astype(F32)
                out[rows, pl.ds(pl.multiple_of(block * width, width), width)] = (
                    ref[side, rows, :].astype(F32) * scale * gain
                ).astype(BF16)
    for step, ref in zip(RING, parts):
        for side in range(2):
            block = origin(x, step) * 2 + (1 - c if side else c)
            gain_two[block] = ref[side, count + 8 : count + 16, :]


def origin(here, step):
    return (here + (4 - step)) & 3


def fill_rows(weight, parts, y, z):
    for step, part in zip(RING, parts):
        for at, less in enumerate(RING):
            for far in range(4):
                start = pl.multiple_of(((far * 4 + origin(z, less)) * 4 + origin(y, step)) * PIECE, PIECE)
                came = (at * 4 + far) * PIECE
                weight[pl.ds(start, PIECE), :] = part[came : came + PIECE, :]


def first_kernel(place, normed, p0, p1, p2, p3, act_u, act_v, sums, weight):
    width = act_u.shape[1]
    fill_rows(weight, (p0, p1, p2, p3), place[2], place[3])
    for part in range(normed.shape[0] // SEQ_LEN):
        rows = pl.ds(part * SEQ_LEN, SEQ_LEN)
        both = gelu(jnp.dot(normed[rows, :], weight[...], preferred_element_type=F32))
        act_u[rows, :] = both[:, :width]
        value = both[:, width:]
        act_v[rows, :] = value
        once = sum(value[:, k : k + 128] for k in range(0, width, 128))
        twice = sum(value[:, k : k + 128] * value[:, k : k + 128] for k in range(0, width, 128))
        sums[0:1, rows] = jnp.sum(once.T, axis=0, keepdims=True)
        sums[1:2, rows] = jnp.sum(twice.T, axis=0, keepdims=True)


def mix_kernel(place, act_v, act_u, stats, gain, shift, mix, bias, p0, p1, p2, p3, give, keep, weight, gated):
    width = act_v.shape[1]
    fill_rows(weight, (p0, p1, p2, p3), place[2], place[3])
    full = width * stats.shape[0]
    i = lax.broadcasted_iota(jnp.int32, (BLOCK, BLOCK), 0)
    j = lax.broadcasted_iota(jnp.int32, (BLOCK, BLOCK), 1)
    visible = (i >= SEGMENT) | (j < SEGMENT)
    total = stats[0]
    for k in range(1, stats.shape[0]):
        total = total + stats[k]
    center_row = total[0:1] / full
    spread_row = total[1:2] / full - center_row * center_row
    scale_row = lax.rsqrt(spread_row + EPS)
    biases = [jnp.broadcast_to(bias[g : g + 1, :].astype(F32), (BLOCK, BLOCK)).T for g in range(width // GROUP_DIM)]
    for block in range(act_v.shape[0] // BLOCK):
        rows = pl.ds(block * BLOCK, BLOCK)
        at = slice(block * BLOCK, (block + 1) * BLOCK)
        center = jnp.broadcast_to(center_row[:, at], (BLOCK, BLOCK)).T
        scale = jnp.broadcast_to(scale_row[:, at], (BLOCK, BLOCK)).T
        for g in range(width // GROUP_DIM):
            cols = slice(g * GROUP_DIM, (g + 1) * GROUP_DIM)
            mixed = ((act_v[rows, cols] - center) * scale * gain[:, cols].astype(F32) + shift[:, cols].astype(F32)).astype(BF16)
            seen = jnp.where(visible, mix[g].astype(F32), 0.0).astype(BF16)
            spatial = jnp.dot(seen, mixed, preferred_element_type=F32) + biases[g]
            gated[rows, cols] = (act_u[rows, cols] * spatial).astype(BF16)
    c = place[1]
    for out, side in ((give, 1 - c), (keep, c)):
        for x in range(out.shape[0]):
            start = pl.multiple_of((2 * x + side) * width, width)
            columns = weight[pl.ds(start, width), :]
            out[x] = lax.dot_general(
                gated[...], columns, (((1,), (1,)), ((), ())), preferred_element_type=F32
            ).astype(BF16)


def shifted(value, by):
    row = lax.broadcasted_iota(jnp.int32, value.shape, 0)
    return jnp.where(row >= by, pltpu.roll(value, by, 0), 0.0)


def taps(value, weights):
    value = value.astype(BF16).astype(F32)
    return (shifted(value, 2) * weights[0:1] + shifted(value, 1) * weights[1:2]) + value * weights[2:3]


def ffn_kernel(place, mine, other, gain, late_hbm, conv_gate, conv_value, give, keep, normed, hidden, late, done):
    width = mine.shape[2]
    ff = conv_gate.shape[1]
    c = place[1]
    copies = [
        pltpu.make_async_copy(late_hbm.at[:, pl.ds(k * ff, ff)], late.at[:, pl.ds(k * ff, ff)], done.at[k])
        for k in range(3)
    ]
    for copy in copies:
        copy.start()
    for part in range(mine.shape[1] // BLOCK):
        rows = pl.ds(part * BLOCK, BLOCK)
        squares = jnp.zeros((BLOCK, width), F32)
        for ref in (mine, other):
            for x in range(4):
                value = ref[x, rows, :].astype(F32)
                squares = squares + value * value
        scale = lax.rsqrt(jnp.sum(squares, axis=1, keepdims=True) / (8 * width) + EPS)
        for side, ref in ((c, mine), (1 - c, other)):
            for x in range(4):
                block = 2 * x + side
                row = gain[block, 0:1, :].astype(F32)
                normed[rows, pl.ds(pl.multiple_of(block * width, width), width)] = (
                    ref[x, rows, :].astype(F32) * scale * row
                ).astype(BF16)
    for part in range(mine.shape[1] // SEQ_LEN):
        rows = pl.ds(part * SEQ_LEN, SEQ_LEN)
        if part == 0:
            copies[0].wait()
        gate = jnp.dot(normed[rows, :], late[:, 0:ff], preferred_element_type=F32)
        if part == 0:
            copies[1].wait()
        value = jnp.dot(normed[rows, :], late[:, ff : 2 * ff], preferred_element_type=F32)
        conv_g = taps(gate, conv_gate[...].astype(F32))
        conv_v = taps(value, conv_value[...].astype(F32))
        hidden[rows, :] = (conv_g * jax.nn.sigmoid(conv_g) * conv_v).astype(BF16)
    copies[2].wait()
    for out, side in ((give, 1 - c), (keep, c)):
        for x in range(out.shape[0]):
            start = pl.multiple_of((2 * x + side) * width, width)
            columns = late[pl.ds(start, width), 2 * ff : 3 * ff]
            out[x] = lax.dot_general(
                hidden[...], columns, (((1,), (1,)), ((), ())), preferred_element_type=F32
            ).astype(BF16)


def gelu(value):
    return 0.5 * value * (1.0 + lax.erf(value * SQRT_HALF))


def shape(dims, dtype):
    return jax.ShapeDtypeStruct(dims, dtype)


def room(mebibytes):
    return pltpu.CompilerParams(vmem_limit_bytes=mebibytes << 20)


def summed_at_owner(give, keep):
    pair = (keep.astype(F32) + other_core(give).astype(F32)).astype(BF16)
    arrived = lax.all_to_all(pair, "x", split_axis=0, concat_axis=0, tiled=True)
    return arrived.astype(F32).sum(axis=0)


def on_device(
    tokens,
    norm_gain,
    proj_u,
    proj_v,
    layer_gain,
    layer_shift,
    mix_weight,
    mix_bias,
    proj_out,
    ffn_gain,
    ffn_gate,
    ffn_value,
    conv_gate,
    conv_value,
    proj_down,
):
    da = proj_u.shape[1]
    ff = ffn_gate.shape[1]
    row_count = tokens.shape[0]

    early = jnp.concatenate([proj_u, proj_v, proj_out.T], axis=1)
    early_far = everyones(early, "zh").reshape(-1, early.shape[1])
    early_z = jnp.concatenate(round_ring(early_far, Z), axis=0)
    early_parts = round_ring(early_z[:, : 2 * da], "y")
    out_parts = round_ring(early_z[:, 2 * da :], "y")

    late = jnp.concatenate([ffn_gate, ffn_value, proj_down.T], axis=1)
    padded = jnp.pad(late, ((0, 2 * late.shape[0]), (0, 0)))
    late_y = lax.all_gather(padded, "y", axis=0)[:, : late.shape[0]].reshape(-1, late.shape[1])
    late_all = lax.all_gather(after(late_y, early_far), Z, axis=0, tiled=True)

    packed = jnp.concatenate([tokens, jnp.broadcast_to(norm_gain, (8, da)), jnp.broadcast_to(ffn_gain, (8, da))], axis=0)
    pair = jnp.stack([packed, other_core(packed)])
    token_parts = round_ring(pair, "x")
    place = jnp.stack([lax.axis_index(name).astype(jnp.int32) for name in ("x", "c", "y", "zl")])
    model = proj_u.shape[0] * lax.axis_size(FS)
    tp = lax.axis_size(TP)
    normed, gain_two = pl.pallas_call(
        norm_kernel,
        in_specs=[SMEM] + [VMEM] * 4,
        out_specs=[VMEM] * 2,
        out_shape=[shape((row_count, model), BF16), shape((tp, 8, da), BF16)],
        name="norm",
        compiler_params=room(12),
    )(place, *token_parts)

    act_u, act_v, sums = pl.pallas_call(
        first_kernel,
        in_specs=[SMEM] + [VMEM] * 5,
        out_specs=[VMEM] * 3,
        out_shape=[shape((row_count, da), F32)] * 2 + [shape((2, row_count), F32)],
        scratch_shapes=[pltpu.VMEM((model, 2 * da), BF16)],
        name="first",
        compiler_params=room(14),
    )(place, normed, *early_parts)
    stats = everyones(sums, TP)
    blocks = [shape((lax.axis_size("x"), row_count, da), BF16)] * 2
    give, keep = pl.pallas_call(
        mix_kernel,
        in_specs=[SMEM] + [VMEM] * 11,
        out_specs=[VMEM] * 2,
        out_shape=blocks,
        scratch_shapes=[pltpu.VMEM((model, da), BF16), pltpu.VMEM((row_count, da), BF16)],
        name="mix",
        compiler_params=room(16),
    )(
        place,
        act_v,
        act_u,
        stats,
        layer_gain[None],
        layer_shift[None],
        mix_weight,
        mix_bias,
        *out_parts,
    )
    stream = (tokens.astype(F32) + summed_at_owner(give, keep)).astype(BF16)
    mine = everyones(stream, "x")
    give, keep = pl.pallas_call(
        ffn_kernel,
        in_specs=[SMEM] + [VMEM] * 3 + [HBM] + [VMEM] * 2,
        out_specs=[VMEM] * 2,
        out_shape=blocks,
        scratch_shapes=[pltpu.VMEM((row_count, model), BF16), pltpu.VMEM((row_count, ff), BF16), pltpu.VMEM(late_all.shape, BF16), pltpu.SemaphoreType.DMA((3,))],
        name="ffn",
        compiler_params=room(47),
    )(
        place,
        mine,
        other_core(mine),
        gain_two,
        late_all,
        conv_gate,
        conv_value,
    )
    return (stream.astype(F32) + summed_at_owner(give, keep)).astype(BF16)


def solution(mesh):
    split = Mesh(mesh.devices.reshape(4, 4, 4, 4, 2), ("zh", "zl", "y", "x", "c"))
    placed = (
        P(FS, TP),
        P(TP),
        P(FS, TP),
        P(FS, TP),
        P(TP),
        P(TP),
        P(TP, None, None),
        P(TP, None),
        P(TP, FS),
        P(TP),
        P(FS, TP),
        P(FS, TP),
        P(None, TP),
        P(None, TP),
        P(TP, FS),
    )

    return jax.shard_map(on_device, mesh=split, in_specs=placed, out_specs=P(FS, TP), check_vma=False)
```

```python
import jax
import jax.numpy as jnp
from jax import lax
from jax.experimental import pallas as pl
from jax.experimental.pallas import tpu as pltpu
from jax.sharding import Mesh
from jax.sharding import PartitionSpec as P

GROUP_DIM = 128
BLOCK = 128
SEGMENT = 64
SEQ_LEN = 256
Z = ("zh", "zl")
FS = ("zh", "zl", "y")
TP = ("x", "c")
EPS = 1e-06
F32 = jnp.float32
BF16 = jnp.bfloat16
SWAP = [(0, 1), (1, 0)]
RING = (0, 2, 1, 3)
PIECE = 32
HBM = pl.BlockSpec(memory_space=pltpu.HBM)
SQRT_HALF = 0.7071067811865476
VMEM = pl.BlockSpec(memory_space=pltpu.VMEM)
SMEM = pl.BlockSpec(memory_space=pltpu.SMEM)


def everyones(shard, axis):
    copies = jnp.broadcast_to(shard, (lax.axis_size(axis), *shard.shape))
    return lax.all_to_all(copies, axis, split_axis=0, concat_axis=0, tiled=True)


def other_core(value):
    return lax.ppermute(value, "c", SWAP)


def after(value, *first):
    return lax.optimization_barrier((value, *first))[0]


def round_ring(shard, axis):
    size = lax.axis_size(axis)
    steps = (2, 1, size - 1)
    return [shard] + [lax.ppermute(shard, axis, [(i, (i + step) % size) for i in range(size)]) for step in steps]


def norm_kernel(place, p0, p1, p2, p3, out, gain_two):
    parts = (p0, p1, p2, p3)
    count, width = p0.shape[1] - 16, p0.shape[2]
    x, c = place[0], place[1]
    for part in range(count // BLOCK):
        rows = pl.ds(part * BLOCK, BLOCK)
        squares = jnp.zeros((BLOCK, width), F32)
        for ref in parts:
            for side in range(2):
                value = ref[side, rows, :].astype(F32)
                squares = squares + value * value
        scale = lax.rsqrt(jnp.sum(squares, axis=1, keepdims=True) / (8 * width) + EPS)
        for step, ref in zip(RING, parts):
            for side in range(2):
                block = origin(x, step) * 2 + (1 - c if side else c)
                gain = ref[side, count : count + 1, :].astype(F32)
                out[rows, pl.ds(pl.multiple_of(block * width, width), width)] = (
                    ref[side, rows, :].astype(F32) * scale * gain
                ).astype(BF16)
    for step, ref in zip(RING, parts):
        for side in range(2):
            block = origin(x, step) * 2 + (1 - c if side else c)
            gain_two[block] = ref[side, count + 8 : count + 16, :]


def origin(here, step):
    return (here + (4 - step)) & 3


def fill_rows(weight, parts, y, z):
    for step, part in zip(RING, parts):
        for at, less in enumerate(RING):
            for far in range(4):
                start = pl.multiple_of(((far * 4 + origin(z, less)) * 4 + origin(y, step)) * PIECE, PIECE)
                came = (at * 4 + far) * PIECE
                weight[pl.ds(start, PIECE), :] = part[came : came + PIECE, :]


def first_kernel(place, normed, p0, p1, p2, p3, act_v, sums, weight):
    width = act_v.shape[1]
    fill_rows(weight, (p0, p1, p2, p3), place[2], place[3])
    for part in range(normed.shape[0] // SEQ_LEN):
        rows = pl.ds(part * SEQ_LEN, SEQ_LEN)
        value = gelu(jnp.dot(normed[rows, :], weight[...], preferred_element_type=F32))
        act_v[rows, :] = value
        once = sum(value[:, k : k + 128] for k in range(0, width, 128))
        twice = sum(value[:, k : k + 128] * value[:, k : k + 128] for k in range(0, width, 128))
        sums[0:1, rows] = jnp.sum(once.T, axis=0, keepdims=True)
        sums[1:2, rows] = jnp.sum(twice.T, axis=0, keepdims=True)


def mix_kernel(place, normed, act_v, stats, gain, shift, mix, bias, p0, p1, p2, p3, give, keep, weight, act_u, gated):
    width = act_v.shape[1]
    fill_rows(weight, (p0, p1, p2, p3), place[2], place[3])
    for part in range(normed.shape[0] // SEQ_LEN):
        rows = pl.ds(part * SEQ_LEN, SEQ_LEN)
        act_u[rows, :] = gelu(jnp.dot(normed[rows, :], weight[:, :width], preferred_element_type=F32))
    full = width * stats.shape[0]
    i = lax.broadcasted_iota(jnp.int32, (BLOCK, BLOCK), 0)
    j = lax.broadcasted_iota(jnp.int32, (BLOCK, BLOCK), 1)
    visible = (i >= SEGMENT) | (j < SEGMENT)
    total = stats[0]
    for k in range(1, stats.shape[0]):
        total = total + stats[k]
    center_row = total[0:1] / full
    spread_row = total[1:2] / full - center_row * center_row
    scale_row = lax.rsqrt(spread_row + EPS)
    biases = [jnp.broadcast_to(bias[g : g + 1, :].astype(F32), (BLOCK, BLOCK)).T for g in range(width // GROUP_DIM)]
    for block in range(act_v.shape[0] // BLOCK):
        rows = pl.ds(block * BLOCK, BLOCK)
        at = slice(block * BLOCK, (block + 1) * BLOCK)
        center = jnp.broadcast_to(center_row[:, at], (BLOCK, BLOCK)).T
        scale = jnp.broadcast_to(scale_row[:, at], (BLOCK, BLOCK)).T
        for g in range(width // GROUP_DIM):
            cols = slice(g * GROUP_DIM, (g + 1) * GROUP_DIM)
            mixed = ((act_v[rows, cols] - center) * scale * gain[:, cols].astype(F32) + shift[:, cols].astype(F32)).astype(BF16)
            seen = jnp.where(visible, mix[g].astype(F32), 0.0).astype(BF16)
            spatial = jnp.dot(seen, mixed, preferred_element_type=F32) + biases[g]
            gated[rows, cols] = (act_u[rows, cols] * spatial).astype(BF16)
    c = place[1]
    for out, side in ((give, 1 - c), (keep, c)):
        for x in range(out.shape[0]):
            start = pl.multiple_of((2 * x + side) * width, width)
            columns = weight[pl.ds(start, width), width : 2 * width]
            out[x] = lax.dot_general(
                gated[...], columns, (((1,), (1,)), ((), ())), preferred_element_type=F32
            ).astype(BF16)


def shifted(value, by):
    row = lax.broadcasted_iota(jnp.int32, value.shape, 0)
    return jnp.where(row >= by, pltpu.roll(value, by, 0), 0.0)


def taps(value, weights):
    value = value.astype(BF16).astype(F32)
    return (shifted(value, 2) * weights[0:1] + shifted(value, 1) * weights[1:2]) + value * weights[2:3]


def ffn_kernel(place, mine, other, gain, late_hbm, conv_gate, conv_value, give, keep, normed, hidden, late, done):
    width = mine.shape[2]
    ff = conv_gate.shape[1]
    c = place[1]
    copies = [
        pltpu.make_async_copy(late_hbm.at[:, pl.ds(k * ff, ff)], late.at[:, pl.ds(k * ff, ff)], done.at[k])
        for k in range(3)
    ]
    copies[0].start()
    for part in range(mine.shape[1] // BLOCK):
        if part == 3:
            copies[1].start()
        rows = pl.ds(part * BLOCK, BLOCK)
        squares = jnp.zeros((BLOCK, width), F32)
        for ref in (mine, other):
            for x in range(4):
                value = ref[x, rows, :].astype(F32)
                squares = squares + value * value
        scale = lax.rsqrt(jnp.sum(squares, axis=1, keepdims=True) / (8 * width) + EPS)
        for side, ref in ((c, mine), (1 - c, other)):
            for x in range(4):
                block = 2 * x + side
                row = gain[block, 0:1, :].astype(F32)
                normed[rows, pl.ds(pl.multiple_of(block * width, width), width)] = (
                    ref[x, rows, :].astype(F32) * scale * row
                ).astype(BF16)
    for part in range(mine.shape[1] // SEQ_LEN):
        rows = pl.ds(part * SEQ_LEN, SEQ_LEN)
        if part == 0:
            copies[0].wait()
        gate = jnp.dot(normed[rows, :], late[:, 0:ff], preferred_element_type=F32)
        if part == 0:
            copies[2].start()
            copies[1].wait()
        value = jnp.dot(normed[rows, :], late[:, ff : 2 * ff], preferred_element_type=F32)
        conv_g = taps(gate, conv_gate[...].astype(F32))
        conv_v = taps(value, conv_value[...].astype(F32))
        hidden[rows, :] = (conv_g * jax.nn.sigmoid(conv_g) * conv_v).astype(BF16)
    copies[2].wait()
    for out, side in ((give, 1 - c), (keep, c)):
        for x in range(out.shape[0]):
            start = pl.multiple_of((2 * x + side) * width, width)
            columns = late[pl.ds(start, width), 2 * ff : 3 * ff]
            out[x] = lax.dot_general(
                hidden[...], columns, (((1,), (1,)), ((), ())), preferred_element_type=F32
            ).astype(BF16)


def gelu(value):
    return 0.5 * value * (1.0 + lax.erf(value * SQRT_HALF))


def shape(dims, dtype):
    return jax.ShapeDtypeStruct(dims, dtype)


def room(mebibytes):
    return pltpu.CompilerParams(vmem_limit_bytes=mebibytes << 20)


def summed_at_owner(give, keep):
    pair = (keep.astype(F32) + other_core(give).astype(F32)).astype(BF16)
    arrived = lax.all_to_all(pair, "x", split_axis=0, concat_axis=0, tiled=True)
    return arrived.astype(F32).sum(axis=0)


def on_device(
    tokens,
    norm_gain,
    proj_u,
    proj_v,
    layer_gain,
    layer_shift,
    mix_weight,
    mix_bias,
    proj_out,
    ffn_gain,
    ffn_gate,
    ffn_value,
    conv_gate,
    conv_value,
    proj_down,
):
    da = proj_u.shape[1]
    ff = ffn_gate.shape[1]
    row_count = tokens.shape[0]

    early = jnp.concatenate([proj_v, proj_u, proj_out.T], axis=1)
    early_far = everyones(early, "zh").reshape(-1, early.shape[1])
    early_z = jnp.concatenate(round_ring(early_far, Z), axis=0)
    early_v, early_rest = lax.optimization_barrier((early_z[:, :da], early_z[:, da:]))
    early_parts = round_ring(early_v, "y")
    out_parts = round_ring(early_rest, "y")

    late = jnp.concatenate([ffn_gate, ffn_value, proj_down.T], axis=1)
    padded = jnp.pad(late, ((0, 2 * late.shape[0]), (0, 0)))
    late_y = lax.all_gather(padded, "y", axis=0)[:, : late.shape[0]].reshape(-1, late.shape[1])
    late_all = lax.all_gather(after(late_y, early_far), Z, axis=0, tiled=True)

    packed = jnp.concatenate([tokens, jnp.broadcast_to(norm_gain, (8, da)), jnp.broadcast_to(ffn_gain, (8, da))], axis=0)
    pair = jnp.stack([packed, other_core(packed)])
    token_parts = round_ring(pair, "x")
    place = jnp.stack([lax.axis_index(name).astype(jnp.int32) for name in ("x", "c", "y", "zl")])
    model = proj_u.shape[0] * lax.axis_size(FS)
    tp = lax.axis_size(TP)
    normed, gain_two = pl.pallas_call(
        norm_kernel,
        in_specs=[SMEM] + [VMEM] * 4,
        out_specs=[VMEM] * 2,
        out_shape=[shape((row_count, model), BF16), shape((tp, 8, da), BF16)],
        name="norm",
        compiler_params=room(12),
    )(place, *token_parts)

    act_v, sums = pl.pallas_call(
        first_kernel,
        in_specs=[SMEM] + [VMEM] * 5,
        out_specs=[VMEM] * 2,
        out_shape=[shape((row_count, da), F32), shape((2, row_count), F32)],
        scratch_shapes=[pltpu.VMEM((model, da), BF16)],
        name="first",
        compiler_params=room(14),
    )(place, normed, *early_parts)
    stats = everyones(sums, TP)
    blocks = [shape((lax.axis_size("x"), row_count, da), BF16)] * 2
    give, keep = pl.pallas_call(
        mix_kernel,
        in_specs=[SMEM] + [VMEM] * 11,
        out_specs=[VMEM] * 2,
        out_shape=blocks,
        scratch_shapes=[
            pltpu.VMEM((model, 2 * da), BF16),
            pltpu.VMEM((row_count, da), F32),
            pltpu.VMEM((row_count, da), BF16),
        ],
        name="mix",
        compiler_params=room(16),
    )(
        place,
        normed,
        act_v,
        stats,
        layer_gain[None],
        layer_shift[None],
        mix_weight,
        mix_bias,
        *out_parts,
    )
    stream = (tokens.astype(F32) + summed_at_owner(give, keep)).astype(BF16)
    mine = everyones(stream, "x")
    give, keep = pl.pallas_call(
        ffn_kernel,
        in_specs=[SMEM] + [VMEM] * 3 + [HBM] + [VMEM] * 2,
        out_specs=[VMEM] * 2,
        out_shape=blocks,
        scratch_shapes=[pltpu.VMEM((row_count, model), BF16), pltpu.VMEM((row_count, ff), BF16), pltpu.VMEM(late_all.shape, BF16), pltpu.SemaphoreType.DMA((3,))],
        name="ffn",
        compiler_params=room(47),
    )(
        place,
        mine,
        other_core(mine),
        gain_two,
        late_all,
        conv_gate,
        conv_value,
    )
    return (stream.astype(F32) + summed_at_owner(give, keep)).astype(BF16)


def solution(mesh):
    split = Mesh(mesh.devices.reshape(4, 4, 4, 4, 2), ("zh", "zl", "y", "x", "c"))
    placed = (
        P(FS, TP),
        P(TP),
        P(FS, TP),
        P(FS, TP),
        P(TP),
        P(TP),
        P(TP, None, None),
        P(TP, None),
        P(TP, FS),
        P(TP),
        P(FS, TP),
        P(FS, TP),
        P(None, TP),
        P(None, TP),
        P(TP, FS),
    )

    return jax.shard_map(on_device, mesh=split, in_specs=placed, out_specs=P(FS, TP), check_vma=False)
```

```python
import jax
import jax.numpy as jnp
from jax import lax
from jax.experimental import pallas as pl
from jax.experimental.pallas import tpu as pltpu
from jax.sharding import Mesh
from jax.sharding import PartitionSpec as P

GROUP_DIM = 128
BLOCK = 128
SEGMENT = 64
SEQ_LEN = 256
Z = ("zh", "zl")
FS = ("zh", "zl", "y")
TP = ("x", "c")
EPS = 1e-06
F32 = jnp.float32
BF16 = jnp.bfloat16
SWAP = [(0, 1), (1, 0)]
RING = (0, 2, 1, 3)
PIECE = 32
HBM = pl.BlockSpec(memory_space=pltpu.HBM)
SQRT_HALF = 0.7071067811865476
VMEM = pl.BlockSpec(memory_space=pltpu.VMEM)
SMEM = pl.BlockSpec(memory_space=pltpu.SMEM)


def everyones(shard, axis):
    copies = jnp.broadcast_to(shard, (lax.axis_size(axis), *shard.shape))
    return lax.all_to_all(copies, axis, split_axis=0, concat_axis=0, tiled=True)


def other_core(value):
    return lax.ppermute(value, "c", SWAP)


def after(value, *first):
    return lax.optimization_barrier((value, *first))[0]


def round_ring(shard, axis):
    size = lax.axis_size(axis)
    steps = (2, 1, size - 1)
    return [shard] + [lax.ppermute(shard, axis, [(i, (i + step) % size) for i in range(size)]) for step in steps]


def norm_kernel(place, p0, p1, p2, p3, out, gain_two):
    parts = (p0, p1, p2, p3)
    count, width = p0.shape[1] - 16, p0.shape[2]
    x, c = place[0], place[1]
    for part in range(count // BLOCK):
        rows = pl.ds(part * BLOCK, BLOCK)
        squares = jnp.zeros((BLOCK, width), F32)
        for ref in parts:
            for side in range(2):
                value = ref[side, rows, :].astype(F32)
                squares = squares + value * value
        scale = lax.rsqrt(jnp.sum(squares, axis=1, keepdims=True) / (8 * width) + EPS)
        for step, ref in zip(RING, parts):
            for side in range(2):
                block = origin(x, step) * 2 + (1 - c if side else c)
                gain = ref[side, count : count + 1, :].astype(F32)
                out[rows, pl.ds(pl.multiple_of(block * width, width), width)] = (
                    ref[side, rows, :].astype(F32) * scale * gain
                ).astype(BF16)
    for step, ref in zip(RING, parts):
        for side in range(2):
            block = origin(x, step) * 2 + (1 - c if side else c)
            gain_two[block] = ref[side, count + 8 : count + 16, :]


def origin(here, step):
    return (here + (4 - step)) & 3


def fill_rows(weight, parts, y, z):
    for step, part in zip(RING, parts):
        for at, less in enumerate(RING):
            for far in range(4):
                start = pl.multiple_of(((far * 4 + origin(z, less)) * 4 + origin(y, step)) * PIECE, PIECE)
                came = (at * 4 + far) * PIECE
                weight[pl.ds(start, PIECE), :] = part[came : came + PIECE, :]


def first_kernel(place, normed, p0, p1, p2, p3, act_v, sums, weight):
    width = act_v.shape[1]
    fill_rows(weight, (p0, p1, p2, p3), place[2], place[3])
    for part in range(normed.shape[0] // SEQ_LEN):
        rows = pl.ds(part * SEQ_LEN, SEQ_LEN)
        value = gelu(jnp.dot(normed[rows, :], weight[...], preferred_element_type=F32))
        act_v[rows, :] = value
        once = sum(value[:, k : k + 128] for k in range(0, width, 128))
        twice = sum(value[:, k : k + 128] * value[:, k : k + 128] for k in range(0, width, 128))
        sums[0:1, rows] = jnp.sum(once.T, axis=0, keepdims=True)
        sums[1:2, rows] = jnp.sum(twice.T, axis=0, keepdims=True)


def mix_kernel(place, normed, act_v, stats, gain, shift, mix, bias, p0, p1, p2, p3, give, keep, weight, act_u, gated):
    width = act_v.shape[1]
    fill_rows(weight, (p0, p1, p2, p3), place[2], place[3])
    for part in range(normed.shape[0] // SEQ_LEN):
        rows = pl.ds(part * SEQ_LEN, SEQ_LEN)
        act_u[rows, :] = gelu(jnp.dot(normed[rows, :], weight[:, :width], preferred_element_type=F32))
    full = width * stats.shape[0]
    i = lax.broadcasted_iota(jnp.int32, (BLOCK, BLOCK), 0)
    j = lax.broadcasted_iota(jnp.int32, (BLOCK, BLOCK), 1)
    visible = (i >= SEGMENT) | (j < SEGMENT)
    total = stats[0]
    for k in range(1, stats.shape[0]):
        total = total + stats[k]
    center_row = total[0:1] / full
    spread_row = total[1:2] / full - center_row * center_row
    scale_row = lax.rsqrt(spread_row + EPS)
    biases = [jnp.broadcast_to(bias[g : g + 1, :].astype(F32), (BLOCK, BLOCK)).T for g in range(width // GROUP_DIM)]
    for block in range(act_v.shape[0] // BLOCK):
        rows = pl.ds(block * BLOCK, BLOCK)
        at = slice(block * BLOCK, (block + 1) * BLOCK)
        center = jnp.broadcast_to(center_row[:, at], (BLOCK, BLOCK)).T
        scale = jnp.broadcast_to(scale_row[:, at], (BLOCK, BLOCK)).T
        for g in range(width // GROUP_DIM):
            cols = slice(g * GROUP_DIM, (g + 1) * GROUP_DIM)
            mixed = ((act_v[rows, cols] - center) * scale * gain[:, cols].astype(F32) + shift[:, cols].astype(F32)).astype(BF16)
            seen = jnp.where(visible, mix[g].astype(F32), 0.0).astype(BF16)
            spatial = jnp.dot(seen, mixed, preferred_element_type=F32) + biases[g]
            gated[rows, cols] = (act_u[rows, cols] * spatial).astype(BF16)
    c = place[1]
    for out, side in ((give, 1 - c), (keep, c)):
        for x in range(out.shape[0]):
            start = pl.multiple_of((2 * x + side) * width, width)
            columns = weight[pl.ds(start, width), width : 2 * width]
            out[x] = lax.dot_general(
                gated[...], columns, (((1,), (1,)), ((), ())), preferred_element_type=F32
            ).astype(BF16)


def shifted(value, by):
    row = lax.broadcasted_iota(jnp.int32, value.shape, 0)
    return jnp.where(row >= by, pltpu.roll(value, by, 0), 0.0)


def taps(value, weights):
    value = value.astype(BF16).astype(F32)
    return (shifted(value, 2) * weights[0:1] + shifted(value, 1) * weights[1:2]) + value * weights[2:3]


def ffn_kernel(place, mine, other, gain, late_hbm, conv_gate, conv_value, give, keep, normed, hidden, late, done):
    width = mine.shape[2]
    ff = conv_gate.shape[1]
    c = place[1]
    copies = [
        pltpu.make_async_copy(late_hbm.at[:, pl.ds(k * ff, ff)], late.at[:, pl.ds(k * ff, ff)], done.at[k])
        for k in range(3)
    ]
    for copy in copies:
        copy.start()
    for part in range(mine.shape[1] // SEQ_LEN):
        rows = pl.ds(part * SEQ_LEN, SEQ_LEN)
        squares = jnp.zeros((SEQ_LEN, 1), F32)
        for x in range(mine.shape[0]):
            for ref in (mine, other):
                value = ref[x, rows, :].astype(F32)
                squares = squares + jnp.sum(value * value, axis=1, keepdims=True)
        scale = lax.rsqrt(squares / (2 * mine.shape[0] * width) + EPS)

        def fill(ref, side):
            for x in range(mine.shape[0]):
                at = pl.ds((2 * x + side) * width, width)
                row = gain[2 * x + side, 0:1, :].astype(F32)
                normed[:, at] = (ref[x, rows, :].astype(F32) * scale * row).astype(BF16)

        @pl.when(c == 0)
        def _():
            fill(mine, 0)
            fill(other, 1)

        @pl.when(c == 1)
        def _():
            fill(other, 0)
            fill(mine, 1)

        if part == 0:
            copies[0].wait()
        gate = jnp.dot(normed[...], late[:, 0:ff], preferred_element_type=F32)
        if part == 0:
            copies[1].wait()
        value = jnp.dot(normed[...], late[:, ff : 2 * ff], preferred_element_type=F32)
        conv_g = taps(gate, conv_gate[...].astype(F32))
        conv_v = taps(value, conv_value[...].astype(F32))
        hidden[rows, :] = (conv_g * jax.nn.sigmoid(conv_g) * conv_v).astype(BF16)
    copies[2].wait()
    for out, side in ((give, 1 - c), (keep, c)):
        for x in range(out.shape[0]):
            start = pl.multiple_of((2 * x + side) * width, width)
            columns = late[pl.ds(start, width), 2 * ff : 3 * ff]
            out[x] = lax.dot_general(
                hidden[...], columns, (((1,), (1,)), ((), ())), preferred_element_type=F32
            ).astype(BF16)


def gelu(value):
    return 0.5 * value * (1.0 + lax.erf(value * SQRT_HALF))


def shape(dims, dtype):
    return jax.ShapeDtypeStruct(dims, dtype)


def room(mebibytes):
    return pltpu.CompilerParams(vmem_limit_bytes=mebibytes << 20)


def summed_at_owner(give, keep):
    pair = (keep.astype(F32) + other_core(give).astype(F32)).astype(BF16)
    arrived = lax.all_to_all(pair, "x", split_axis=0, concat_axis=0, tiled=True)
    return arrived.astype(F32).sum(axis=0)


def on_device(
    tokens,
    norm_gain,
    proj_u,
    proj_v,
    layer_gain,
    layer_shift,
    mix_weight,
    mix_bias,
    proj_out,
    ffn_gain,
    ffn_gate,
    ffn_value,
    conv_gate,
    conv_value,
    proj_down,
):
    da = proj_u.shape[1]
    ff = ffn_gate.shape[1]
    row_count = tokens.shape[0]

    early = jnp.concatenate([proj_v, proj_u, proj_out.T], axis=1)
    early_far = everyones(early, "zh").reshape(-1, early.shape[1])
    early_z = jnp.concatenate(round_ring(early_far, Z), axis=0)
    early_v, early_rest = lax.optimization_barrier((early_z[:, :da], early_z[:, da:]))
    early_parts = round_ring(early_v, "y")
    out_parts = round_ring(early_rest, "y")

    late = jnp.concatenate([ffn_gate, ffn_value, proj_down.T], axis=1)
    padded = jnp.pad(late, ((0, 2 * late.shape[0]), (0, 0)))
    late_y = lax.all_gather(padded, "y", axis=0)[:, : late.shape[0]].reshape(-1, late.shape[1])
    late_all = lax.all_gather(after(late_y, early_far), Z, axis=0, tiled=True)

    packed = jnp.concatenate([tokens, jnp.broadcast_to(norm_gain, (8, da)), jnp.broadcast_to(ffn_gain, (8, da))], axis=0)
    pair = jnp.stack([packed, other_core(packed)])
    token_parts = round_ring(pair, "x")
    place = jnp.stack([lax.axis_index(name).astype(jnp.int32) for name in ("x", "c", "y", "zl")])
    model = proj_u.shape[0] * lax.axis_size(FS)
    tp = lax.axis_size(TP)
    normed, gain_two = pl.pallas_call(
        norm_kernel,
        in_specs=[SMEM] + [VMEM] * 4,
        out_specs=[VMEM] * 2,
        out_shape=[shape((row_count, model), BF16), shape((tp, 8, da), BF16)],
        name="norm",
        compiler_params=room(12),
    )(place, *token_parts)

    act_v, sums = pl.pallas_call(
        first_kernel,
        in_specs=[SMEM] + [VMEM] * 5,
        out_specs=[VMEM] * 2,
        out_shape=[shape((row_count, da), F32), shape((2, row_count), F32)],
        scratch_shapes=[pltpu.VMEM((model, da), BF16)],
        name="first",
        compiler_params=room(14),
    )(place, normed, *early_parts)
    stats = everyones(sums, TP)
    blocks = [shape((lax.axis_size("x"), row_count, da), BF16)] * 2
    give, keep = pl.pallas_call(
        mix_kernel,
        in_specs=[SMEM] + [VMEM] * 11,
        out_specs=[VMEM] * 2,
        out_shape=blocks,
        scratch_shapes=[
            pltpu.VMEM((model, 2 * da), BF16),
            pltpu.VMEM((row_count, da), F32),
            pltpu.VMEM((row_count, da), BF16),
        ],
        name="mix",
        compiler_params=room(16),
    )(
        place,
        normed,
        act_v,
        stats,
        layer_gain[None],
        layer_shift[None],
        mix_weight,
        mix_bias,
        *out_parts,
    )
    stream = (tokens.astype(F32) + summed_at_owner(give, keep)).astype(BF16)
    mine = everyones(stream, "x")
    give, keep = pl.pallas_call(
        ffn_kernel,
        in_specs=[SMEM] + [VMEM] * 3 + [HBM] + [VMEM] * 2,
        out_specs=[VMEM] * 2,
        out_shape=blocks,
        scratch_shapes=[pltpu.VMEM((SEQ_LEN, model), BF16), pltpu.VMEM((row_count, ff), BF16), pltpu.VMEM(late_all.shape, BF16), pltpu.SemaphoreType.DMA((3,))],
        name="ffn",
        compiler_params=room(47),
    )(
        place,
        mine,
        other_core(mine),
        gain_two,
        late_all,
        conv_gate,
        conv_value,
    )
    return (stream.astype(F32) + summed_at_owner(give, keep)).astype(BF16)


def solution(mesh):
    split = Mesh(mesh.devices.reshape(4, 4, 4, 4, 2), ("zh", "zl", "y", "x", "c"))
    placed = (
        P(FS, TP),
        P(TP),
        P(FS, TP),
        P(FS, TP),
        P(TP),
        P(TP),
        P(TP, None, None),
        P(TP, None),
        P(TP, FS),
        P(TP),
        P(FS, TP),
        P(FS, TP),
        P(None, TP),
        P(None, TP),
        P(TP, FS),
    )

    return jax.shard_map(on_device, mesh=split, in_specs=placed, out_specs=P(FS, TP), check_vma=False)
```

```python
import jax
import jax.numpy as jnp
from jax import lax
from jax.experimental import pallas as pl
from jax.experimental.pallas import tpu as pltpu
from jax.sharding import Mesh
from jax.sharding import PartitionSpec as P

GROUP_DIM = 128
BLOCK = 128
SEGMENT = 64
SEQ_LEN = 256
Z = ("zh", "zl")
FS = ("zh", "zl", "y")
TP = ("x", "c")
EPS = 1e-06
F32 = jnp.float32
BF16 = jnp.bfloat16
SWAP = [(0, 1), (1, 0)]
RING = (0, 2, 1, 3)
PIECE = 32
HBM = pl.BlockSpec(memory_space=pltpu.HBM)
SQRT_HALF = 0.7071067811865476
VMEM = pl.BlockSpec(memory_space=pltpu.VMEM)
SMEM = pl.BlockSpec(memory_space=pltpu.SMEM)


def everyones(shard, axis):
    copies = jnp.broadcast_to(shard, (lax.axis_size(axis), *shard.shape))
    return lax.all_to_all(copies, axis, split_axis=0, concat_axis=0, tiled=True)


def other_core(value):
    return lax.ppermute(value, "c", SWAP)


def after(value, *first):
    return lax.optimization_barrier((value, *first))[0]


def round_ring(shard, axis):
    size = lax.axis_size(axis)
    steps = (2, 1, size - 1)
    return [shard] + [lax.ppermute(shard, axis, [(i, (i + step) % size) for i in range(size)]) for step in steps]


def norm_kernel(place, p0, p1, p2, p3, out, gain_two):
    parts = (p0, p1, p2, p3)
    count, width = p0.shape[1] - 16, p0.shape[2]
    x, c = place[0], place[1]
    for part in range(count // BLOCK):
        rows = pl.ds(part * BLOCK, BLOCK)
        squares = jnp.zeros((BLOCK, width), F32)
        for ref in parts:
            for side in range(2):
                value = ref[side, rows, :].astype(F32)
                squares = squares + value * value
        scale = lax.rsqrt(jnp.sum(squares, axis=1, keepdims=True) / (8 * width) + EPS)
        for step, ref in zip(RING, parts):
            for side in range(2):
                block = origin(x, step) * 2 + (1 - c if side else c)
                gain = ref[side, count : count + 1, :].astype(F32)
                out[rows, pl.ds(pl.multiple_of(block * width, width), width)] = (
                    ref[side, rows, :].astype(F32) * scale * gain
                ).astype(BF16)
    for step, ref in zip(RING, parts):
        for side in range(2):
            block = origin(x, step) * 2 + (1 - c if side else c)
            gain_two[block] = ref[side, count + 8 : count + 16, :]


def origin(here, step):
    return (here + (4 - step)) & 3


def fill_rows(weight, parts, y, z):
    for step, part in zip(RING, parts):
        for at, less in enumerate(RING):
            for far in range(4):
                start = pl.multiple_of(((far * 4 + origin(z, less)) * 4 + origin(y, step)) * PIECE, PIECE)
                came = (at * 4 + far) * PIECE
                weight[pl.ds(start, PIECE), :] = part[came : came + PIECE, :]


def first_kernel(place, normed, p0, p1, p2, p3, act_u, act_v, sums, weight):
    width = act_u.shape[1]
    fill_rows(weight, (p0, p1, p2, p3), place[2], place[3])
    for part in range(normed.shape[0] // SEQ_LEN):
        rows = pl.ds(part * SEQ_LEN, SEQ_LEN)
        both = gelu(jnp.dot(normed[rows, :], weight[...], preferred_element_type=F32))
        act_u[rows, :] = both[:, :width]
        value = both[:, width:]
        act_v[rows, :] = value
        once = sum(value[:, k : k + 128] for k in range(0, width, 128))
        twice = sum(value[:, k : k + 128] * value[:, k : k + 128] for k in range(0, width, 128))
        sums[0:1, rows] = jnp.sum(once.T, axis=0, keepdims=True)
        sums[1:2, rows] = jnp.sum(twice.T, axis=0, keepdims=True)


def mix_kernel(place, act_v, act_u, stats, gain, shift, mix, bias, p0, p1, p2, p3, give, keep, weight, gated):
    width = act_v.shape[1]
    fill_rows(weight, (p0, p1, p2, p3), place[2], place[3])
    full = width * stats.shape[0]
    i = lax.broadcasted_iota(jnp.int32, (BLOCK, BLOCK), 0)
    j = lax.broadcasted_iota(jnp.int32, (BLOCK, BLOCK), 1)
    visible = (i >= SEGMENT) | (j < SEGMENT)
    total = stats[0]
    for k in range(1, stats.shape[0]):
        total = total + stats[k]
    center_row = total[0:1] / full
    spread_row = total[1:2] / full - center_row * center_row
    scale_row = lax.rsqrt(spread_row + EPS)
    biases = [jnp.broadcast_to(bias[g : g + 1, :].astype(F32), (BLOCK, BLOCK)).T for g in range(width // GROUP_DIM)]
    for block in range(act_v.shape[0] // BLOCK):
        rows = pl.ds(block * BLOCK, BLOCK)
        at = slice(block * BLOCK, (block + 1) * BLOCK)
        center = jnp.broadcast_to(center_row[:, at], (BLOCK, BLOCK)).T
        scale = jnp.broadcast_to(scale_row[:, at], (BLOCK, BLOCK)).T
        for g in range(width // GROUP_DIM):
            cols = slice(g * GROUP_DIM, (g + 1) * GROUP_DIM)
            mixed = ((act_v[rows, cols] - center) * scale * gain[:, cols].astype(F32) + shift[:, cols].astype(F32)).astype(BF16)
            seen = jnp.where(visible, mix[g].astype(F32), 0.0).astype(BF16)
            spatial = jnp.dot(seen, mixed, preferred_element_type=F32) + biases[g]
            gated[rows, cols] = (act_u[rows, cols] * spatial).astype(BF16)
    c = place[1]
    for out, side in ((give, 1 - c), (keep, c)):
        for x in range(out.shape[0]):
            start = pl.multiple_of((2 * x + side) * width, width)
            columns = weight[pl.ds(start, width), :]
            out[x] = lax.dot_general(
                gated[...], columns, (((1,), (1,)), ((), ())), preferred_element_type=F32
            ).astype(BF16)


def shifted(value, by):
    row = lax.broadcasted_iota(jnp.int32, value.shape, 0)
    return jnp.where(row >= by, pltpu.roll(value, by, 0), 0.0)


def taps(value, weights):
    value = value.astype(BF16).astype(F32)
    return (shifted(value, 2) * weights[0:1] + shifted(value, 1) * weights[1:2]) + value * weights[2:3]


def ffn_kernel(place, mine, other, gain, late_hbm, conv_gate, conv_value, give, keep, normed, hidden, late, done):
    width = mine.shape[2]
    ff = conv_gate.shape[1]
    c = place[1]
    copies = [
        pltpu.make_async_copy(late_hbm.at[:, pl.ds(k * ff, ff)], late.at[:, pl.ds(k * ff, ff)], done.at[k])
        for k in range(3)
    ]
    for copy in copies:
        copy.start()
    for part in range(mine.shape[1] // SEQ_LEN):
        rows = pl.ds(part * SEQ_LEN, SEQ_LEN)
        squares = jnp.zeros((SEQ_LEN, 1), F32)
        for x in range(mine.shape[0]):
            for ref in (mine, other):
                value = ref[x, rows, :].astype(F32)
                squares = squares + jnp.sum(value * value, axis=1, keepdims=True)
        scale = lax.rsqrt(squares / (2 * mine.shape[0] * width) + EPS)

        def fill(ref, side):
            for x in range(mine.shape[0]):
                at = pl.ds((2 * x + side) * width, width)
                row = gain[2 * x + side, 0:1, :].astype(F32)
                normed[:, at] = (ref[x, rows, :].astype(F32) * scale * row).astype(BF16)

        @pl.when(c == 0)
        def _():
            fill(mine, 0)
            fill(other, 1)

        @pl.when(c == 1)
        def _():
            fill(other, 0)
            fill(mine, 1)

        if part == 0:
            copies[0].wait()
        gate = jnp.dot(normed[...], late[:, 0:ff], preferred_element_type=F32)
        if part == 0:
            copies[1].wait()
        value = jnp.dot(normed[...], late[:, ff : 2 * ff], preferred_element_type=F32)
        conv_g = taps(gate, conv_gate[...].astype(F32))
        conv_v = taps(value, conv_value[...].astype(F32))
        hidden[rows, :] = (conv_g * jax.nn.sigmoid(conv_g) * conv_v).astype(BF16)
    copies[2].wait()
    for out, side in ((give, 1 - c), (keep, c)):
        for x in range(out.shape[0]):
            start = pl.multiple_of((2 * x + side) * width, width)
            columns = late[pl.ds(start, width), 2 * ff : 3 * ff]
            out[x] = lax.dot_general(
                hidden[...], columns, (((1,), (1,)), ((), ())), preferred_element_type=F32
            ).astype(BF16)


def gelu(value):
    return 0.5 * value * (1.0 + lax.erf(value * SQRT_HALF))


def shape(dims, dtype):
    return jax.ShapeDtypeStruct(dims, dtype)


def room(mebibytes):
    return pltpu.CompilerParams(vmem_limit_bytes=mebibytes << 20)


def summed_at_owner(give, keep):
    pair = (keep.astype(F32) + other_core(give).astype(F32)).astype(BF16)
    arrived = lax.all_to_all(pair, "x", split_axis=0, concat_axis=0, tiled=True)
    return arrived.astype(F32).sum(axis=0)


def on_device(
    tokens,
    norm_gain,
    proj_u,
    proj_v,
    layer_gain,
    layer_shift,
    mix_weight,
    mix_bias,
    proj_out,
    ffn_gain,
    ffn_gate,
    ffn_value,
    conv_gate,
    conv_value,
    proj_down,
):
    da = proj_u.shape[1]
    ff = ffn_gate.shape[1]
    row_count = tokens.shape[0]

    early = jnp.concatenate([proj_u, proj_v, proj_out.T], axis=1)
    early_far = everyones(early, "zh").reshape(-1, early.shape[1])
    early_z = jnp.concatenate(round_ring(early_far, Z), axis=0)
    early_uv, early_out = lax.optimization_barrier((early_z[:, : 2 * da], early_z[:, 2 * da :]))
    early_parts = round_ring(early_uv, "y")
    out_parts = round_ring(early_out, "y")

    late = jnp.concatenate([ffn_gate, ffn_value, proj_down.T], axis=1)
    padded = jnp.pad(late, ((0, 2 * late.shape[0]), (0, 0)))
    late_y = lax.all_gather(padded, "y", axis=0)[:, : late.shape[0]].reshape(-1, late.shape[1])
    late_all = lax.all_gather(after(late_y, early_far), Z, axis=0, tiled=True)

    packed = jnp.concatenate([tokens, jnp.broadcast_to(norm_gain, (8, da)), jnp.broadcast_to(ffn_gain, (8, da))], axis=0)
    pair = jnp.stack([packed, other_core(packed)])
    token_parts = round_ring(pair, "x")
    place = jnp.stack([lax.axis_index(name).astype(jnp.int32) for name in ("x", "c", "y", "zl")])
    model = proj_u.shape[0] * lax.axis_size(FS)
    tp = lax.axis_size(TP)
    normed, gain_two = pl.pallas_call(
        norm_kernel,
        in_specs=[SMEM] + [VMEM] * 4,
        out_specs=[VMEM] * 2,
        out_shape=[shape((row_count, model), BF16), shape((tp, 8, da), BF16)],
        name="norm",
        compiler_params=room(12),
    )(place, *token_parts)

    act_u, act_v, sums = pl.pallas_call(
        first_kernel,
        in_specs=[SMEM] + [VMEM] * 5,
        out_specs=[VMEM] * 3,
        out_shape=[shape((row_count, da), F32)] * 2 + [shape((2, row_count), F32)],
        scratch_shapes=[pltpu.VMEM((model, 2 * da), BF16)],
        name="first",
        compiler_params=room(14),
    )(place, normed, *early_parts)
    stats = everyones(sums, TP)
    blocks = [shape((lax.axis_size("x"), row_count, da), BF16)] * 2
    give, keep = pl.pallas_call(
        mix_kernel,
        in_specs=[SMEM] + [VMEM] * 11,
        out_specs=[VMEM] * 2,
        out_shape=blocks,
        scratch_shapes=[pltpu.VMEM((model, da), BF16), pltpu.VMEM((row_count, da), BF16)],
        name="mix",
        compiler_params=room(16),
    )(
        place,
        act_v,
        act_u,
        stats,
        layer_gain[None],
        layer_shift[None],
        mix_weight,
        mix_bias,
        *out_parts,
    )
    stream = (tokens.astype(F32) + summed_at_owner(give, keep)).astype(BF16)
    mine = everyones(stream, "x")
    give, keep = pl.pallas_call(
        ffn_kernel,
        in_specs=[SMEM] + [VMEM] * 3 + [HBM] + [VMEM] * 2,
        out_specs=[VMEM] * 2,
        out_shape=blocks,
        scratch_shapes=[pltpu.VMEM((SEQ_LEN, model), BF16), pltpu.VMEM((row_count, ff), BF16), pltpu.VMEM(late_all.shape, BF16), pltpu.SemaphoreType.DMA((3,))],
        name="ffn",
        compiler_params=room(47),
    )(
        place,
        mine,
        other_core(mine),
        gain_two,
        late_all,
        conv_gate,
        conv_value,
    )
    return (stream.astype(F32) + summed_at_owner(give, keep)).astype(BF16)


def solution(mesh):
    split = Mesh(mesh.devices.reshape(4, 4, 4, 4, 2), ("zh", "zl", "y", "x", "c"))
    placed = (
        P(FS, TP),
        P(TP),
        P(FS, TP),
        P(FS, TP),
        P(TP),
        P(TP),
        P(TP, None, None),
        P(TP, None),
        P(TP, FS),
        P(TP),
        P(FS, TP),
        P(FS, TP),
        P(None, TP),
        P(None, TP),
        P(TP, FS),
    )

    return jax.shard_map(on_device, mesh=split, in_specs=placed, out_specs=P(FS, TP), check_vma=False)
```
